256 devices in a mesh: grp: 2 (over y), fs: 16 (over z), tp: 8 (over x, core).
Axes of the slice: x: 4, y: 2, z: 16, core: 2. Of those that a mesh axis runs over, the one named last changes fastest.
The devices are a block of a 4x16x16 slice.
Arguments:
- block_source_tensor: bfloat16 [16384, 2048], P(('grp', 'fs'), 'tp'), parts along dimension 0, may hold values from -6 to 6
- attend_initial_norm_gain: float32 [2048], replicated, may hold values from 0.1 to 1.9
- each_channel_group_norm: float32 [8, 256], P('tp'), may hold values from 0.1 to 1.9
- attend_final_norm_gain: float32 [2048], replicated, may hold values from 0.1 to 1.9
- dense_initial_norm_gain: float32 [2048], replicated, may hold values from 0.1 to 1.9
- dense_final_norm_gain: float32 [2048], replicated, may hold values from 0.1 to 1.9
- question_map: bfloat16 [2048, 1024], P('fs', 'tp'), may hold values from -0.125 to 0.125
- address_map: bfloat16 [2048, 1024], P('fs', 'tp'), may hold values from -0.125 to 0.125
- payload_weights_map: bfloat16 [2048, 2048], P('fs', 'tp'), may hold values from -0.125 to 0.125
- fading_left_factor: bfloat16 [2048, 16], replicated, may hold values from -0.125 to 0.125
- fading_right_factor: float32 [16, 1024], P(None, 'tp'), may hold values from -1.5 to 1.5
- fading_valve_constant: float32 [1024], P('tp'), may hold values from 0.05 to 6.2
- sudden_fade_excess: float32 [16384, 1024], P(('grp', 'fs'), 'tp'), parts along dimension 0, may hold values from -0.7 to 0
- combining_map: bfloat16 [2048, 2048], P('tp', 'fs')
- valve_map: bfloat16 [2048, 3072], P('fs', 'tp'), may hold values from -0.125 to 0.125
- widening_map: bfloat16 [2048, 3072], P('fs', 'tp'), may hold values from -0.125 to 0.125
- valve_conv_stencil: bfloat16 [3, 3072], P(None, 'tp'), may hold values from -3.5 to 3.5
- widening_conv_stencil: bfloat16 [3, 3072], P(None, 'tp'), may hold values from -3.5 to 3.5
- narrowing_map: bfloat16 [3072, 2048], P('tp', 'fs')
Outputs:
- layer_out: bfloat16 [16384, 2048], P(('grp', 'fs'), 'tp'), parts along dimension 0
The draws below stay inside these ranges and needn't reach their ends.
There are 2 independent parts, one for each index of `grp`. The reference program is written for one: setup_inputs(seed, part) draws one part's arguments, and reference() takes and returns one part's arrays. A program takes and returns all parts, laid end to end along the dimension named above; an argument that names none is the same for every part. Nothing has to cross between parts.
All inputs are finite; a program needn't handle non-finite values.
Results may differ from the reference program's by a relative error of at most 0.019.
Values may be sent and summed in bfloat16 or wider, within the bound.
A program may use at most 64 MiB of HBM per device.

```python
import math
import jax
import jax.numpy as jnp
from jax import lax

D = 2048
HEADS = 8
KEY_DIM = 128
VALUE_DIM = 256
FFN_UNITS = 3072
RANK = 16
TAPS = 3
BLOCK = 16
SEQ = 512
TOKENS = 8192
QK_WIDTH = 1024
V_WIDTH = 2048
N_TP = 8


def rising_columns(key, row_count, column_count, ceiling):
    noise_key, jitter_key = jax.random.split(key)
    ramp = ceiling ** (jnp.arange(column_count, dtype=jnp.float32) / column_count)
    jitter = jnp.exp(jax.random.uniform(jitter_key, (column_count,), jnp.float32, -0.35, 0.35))
    noise = jnp.clip(jax.random.normal(noise_key, (row_count, column_count), jnp.float32), -4.0, 4.0)
    return (noise * (ramp * jitter) * row_count ** (-0.5)).astype(jnp.bfloat16)


def draw_combining_map(key, part):
    ceiling = 10.0
    return rising_columns(jax.random.fold_in(key, 11), V_WIDTH, D, ceiling)


def draw_narrowing_map(key, part):
    ceiling = 10.0
    return rising_columns(jax.random.fold_in(key, 23), FFN_UNITS, D, ceiling)


def draw_fading_valve_constant(key, part):
    head_key, slow_key, fast_key = jax.random.split(jax.random.fold_in(key, 37), 3)
    slow_limit = 5
    slow_heads = jax.random.randint(head_key, (HEADS, 1), 0, 10) < slow_limit
    slow_rate = jnp.exp(jax.random.uniform(slow_key, (HEADS, KEY_DIM), jnp.float32, math.log(0.3), math.log(2.0))) / SEQ
    fast_rate = jnp.exp(-jax.random.uniform(fast_key, (HEADS, KEY_DIM), jnp.float32, math.log(30.0), math.log(100.0)))
    step_rate = jnp.where(slow_heads, slow_rate, fast_rate)
    return (-jnp.log(jnp.expm1(16.0 * step_rate))).reshape(QK_WIDTH)


def draw_sudden_fade_excess(key, part):
    spots_key, amount_key = jax.random.split(jax.random.fold_in(key, 53))
    sequences = TOKENS // SEQ
    spots = jax.random.randint(spots_key, (sequences, 3), 0, SEQ)
    struck = jnp.any(jnp.arange(SEQ)[None, None, :] == spots[:, :, None], axis=1)
    amounts = jax.random.uniform(amount_key, (TOKENS, QK_WIDTH), jnp.float32, math.log(0.5), math.log(0.8))
    return jnp.where(struck.reshape(TOKENS, 1), amounts, 0.0)


def block_scale(rng, shape, pieces, least, top_value):
    def one(position, shards_of):
        heights = jax.random.uniform(jax.random.fold_in(jax.random.fold_in(rng, 6), position), (shards_of,), jnp.float32, least / len(pieces), top_value / len(pieces))
        return jnp.repeat(jnp.exp(heights), shape[position] // shards_of).reshape((-1,) + (1,) * (len(shape) - position - 1))

    level = one(*pieces[0])
    for cut in pieces[1:]:
        level = level * one(*cut)
    return level


def normal_values(stream_key, shape, deviation, most, cuts=(), kind=jnp.bfloat16):
    entries = jax.random.normal(stream_key, shape, jnp.float32) * deviation
    if len(cuts) > 0:
        entries = block_scale(stream_key, shape, cuts, -0.22, 0.18) * entries
    return jnp.clip(entries, min=-most, max=most).astype(kind)


def setup_inputs(seed: int = 0, part: int = 0) -> dict:
    key_of = jax.random.split(jax.random.key(seed), 20)
    part_splits = jax.random.split(jax.random.fold_in(key_of[19], part), 20)
    return {
        "block_source_tensor": normal_values(part_splits[0], (TOKENS, D), 1.0, 6.0, ((0, 16), (1, 8))),
        "attend_initial_norm_gain": jnp.clip(1.0 + 0.18 * jax.random.normal(key_of[1], (D,), jnp.float32), 0.1, 1.9),
        "each_channel_group_norm": jnp.clip(1.0 + 0.18 * jax.random.normal(key_of[2], (HEADS, VALUE_DIM), jnp.float32), 0.1, 1.9),
        "attend_final_norm_gain": jnp.clip(1.0 + 0.18 * jax.random.normal(key_of[3], (D,), jnp.float32), 0.1, 1.9),
        "dense_initial_norm_gain": jnp.clip(1.0 + 0.18 * jax.random.normal(key_of[4], (D,), jnp.float32), 0.1, 1.9),
        "dense_final_norm_gain": jnp.clip(1.0 + 0.18 * jax.random.normal(key_of[5], (D,), jnp.float32), 0.1, 1.9),
        "question_map": normal_values(key_of[6], (D, QK_WIDTH), D ** -0.5, 0.125, ((0, 16), (1, 8))),
        "address_map": normal_values(key_of[7], (D, QK_WIDTH), D ** -0.5, 0.125, ((0, 16), (1, 8))),
        "payload_weights_map": normal_values(key_of[8], (D, V_WIDTH), D ** -0.5, 0.125, ((0, 16), (1, 8))),
        "fading_left_factor": normal_values(key_of[9], (D, RANK), D ** -0.5, 0.125),
        "fading_right_factor": normal_values(key_of[10], (RANK, QK_WIDTH), RANK ** -0.5, 1.5, ((1, 8),), jnp.float32),
        "fading_valve_constant": draw_fading_valve_constant(jax.random.fold_in(key_of[19], 71), part),
        "sudden_fade_excess": draw_sudden_fade_excess(jax.random.fold_in(jax.random.fold_in(key_of[19], part), 71), part),
        "combining_map": draw_combining_map(jax.random.fold_in(key_of[19], 71), part),
        "valve_map": normal_values(key_of[14], (D, FFN_UNITS), D ** -0.5, 0.125, ((0, 16), (1, 8))),
        "widening_map": normal_values(key_of[15], (D, FFN_UNITS), D ** -0.5, 0.125, ((0, 16), (1, 8))),
        "valve_conv_stencil": normal_values(key_of[16], (TAPS, FFN_UNITS), TAPS ** -0.5, 3.5, ((1, 8),)),
        "widening_conv_stencil": normal_values(key_of[17], (TAPS, FFN_UNITS), TAPS ** -0.5, 3.5, ((1, 8),)),
        "narrowing_map": draw_narrowing_map(jax.random.fold_in(key_of[19], 71), part),
    }


epsilon = 1e-06
valve_steepness = 16.0
careful_evaluation = lax.Precision.HIGHEST

def norm_rows(values, channel_gain):
    return values * lax.rsqrt(lax.optimization_barrier(jnp.mean(values * values, axis=-1, keepdims=True)) + epsilon) * channel_gain

def rounded(values):
    return lax.optimization_barrier(values.astype(jnp.bfloat16)).astype(jnp.float32)

def gated_linear(query_rows, key_rows, value_rows, fading_typical_span):
    length, head_count, key_width = query_rows.shape
    blocks = length // BLOCK
    query_rows = query_rows.reshape(blocks, BLOCK, head_count, key_width)
    key_rows = key_rows.reshape(blocks, BLOCK, head_count, key_width)
    value_rows = value_rows.reshape(blocks, BLOCK, head_count, -1)
    cumulative = jnp.cumsum(fading_typical_span.reshape(blocks, BLOCK, head_count, key_width), axis=1)
    tail_decay = cumulative[:, -1]
    query_in = query_rows * jnp.exp(cumulative)
    key_in = key_rows * jnp.exp(-cumulative)
    key_end = key_rows * jnp.exp(tail_decay[:, None] - cumulative)
    causal = jnp.tril(jnp.ones((BLOCK, BLOCK), dtype=bool))
    scores = jnp.einsum('nthk,nshk->nhts', query_in, key_in, precision=careful_evaluation)
    scores = jnp.where(causal, scores, 0.0)
    inner = jnp.einsum('nhts,nshv->nthv', scores, value_rows, precision=careful_evaluation)
    states = jnp.einsum('nshk,nshv->nhkv', key_end, value_rows, precision=careful_evaluation)

    def combine(earlier, latter):
        return (earlier[0] * latter[0], latter[0][..., None] * earlier[1] + latter[1])
    running = lax.associative_scan(combine, (jnp.exp(tail_decay), states))[1]
    carried = jnp.concatenate([jnp.zeros_like(running[:1]), running[:-1]], axis=0)
    outer = jnp.einsum('nthk,nhkv->nthv', query_in, carried, precision=careful_evaluation)
    return (inner + outer).reshape(length, head_count, -1)

def causal_taps(values, kernel):
    tap_count = kernel.shape[0]
    length = values.shape[-2]
    padded = jnp.pad(values, [(0, 0)] * (values.ndim - 2) + [(tap_count - 1, 0), (0, 0)])
    kernel = kernel.astype(jnp.float32)
    summed = kernel[0] * padded[..., 0:length, :]
    for offset in range(1, tap_count):
        summed = summed + kernel[offset] * padded[..., offset:offset + length, :]
    return summed

def grouped_sum(left_rows, right_rows, groups):
    span_rows = left_rows.shape[1] // groups
    running_sum = jnp.zeros((left_rows.shape[0], right_rows.shape[1]), jnp.float32)
    for group_index in range(groups):
        low_end = group_index * span_rows
        partial_value = jnp.dot(left_rows[:, low_end:low_end + span_rows], right_rows[low_end:low_end + span_rows], preferred_element_type=jnp.float32)
        running_sum = running_sum + rounded(partial_value)
    return running_sum

def reference(block_source_tensor, attend_initial_norm_gain, each_channel_group_norm, attend_final_norm_gain, dense_initial_norm_gain, dense_final_norm_gain, question_map, address_map, payload_weights_map, fading_left_factor, fading_right_factor, fading_valve_constant, sudden_fade_excess, combining_map, valve_map, widening_map, valve_conv_stencil, widening_conv_stencil, narrowing_map):
    sequences = TOKENS // SEQ
    normed = norm_rows(block_source_tensor.astype(jnp.float32), attend_initial_norm_gain).astype(jnp.bfloat16)
    query_rows = rounded(jnp.dot(normed, question_map, preferred_element_type=jnp.float32)) * KEY_DIM ** (-0.5)
    key_rows = rounded(jnp.dot(normed, address_map, preferred_element_type=jnp.float32))
    value_rows = rounded(jnp.dot(normed, payload_weights_map, preferred_element_type=jnp.float32))
    fading_narrow_count = jnp.dot(normed, fading_left_factor, preferred_element_type=jnp.float32)
    fading_typical_span = jax.nn.log_sigmoid(jnp.dot(fading_narrow_count, fading_right_factor, precision=careful_evaluation) + fading_valve_constant) / valve_steepness + sudden_fade_excess

    def per_sequence(packed):
        return gated_linear(*packed)
    shaped = tuple((member.reshape(sequences, SEQ, HEADS, -1) for member in (query_rows, key_rows, value_rows, fading_typical_span)))
    mixed_heads = lax.map(per_sequence, shaped).reshape(TOKENS, HEADS, VALUE_DIM)
    head_out = norm_rows(mixed_heads, each_channel_group_norm).astype(jnp.bfloat16).reshape(TOKENS, V_WIDTH)
    mixed = grouped_sum(head_out, combining_map, N_TP)
    first = (block_source_tensor.astype(jnp.float32) + norm_rows(mixed, attend_final_norm_gain)).astype(jnp.bfloat16)
    ffn_in = norm_rows(first.astype(jnp.float32), dense_initial_norm_gain).astype(jnp.bfloat16)
    gate_pre = jnp.dot(ffn_in, valve_map, preferred_element_type=jnp.float32).reshape(sequences, SEQ, FFN_UNITS)
    up_pre = jnp.dot(ffn_in, widening_map, preferred_element_type=jnp.float32).reshape(sequences, SEQ, FFN_UNITS)
    hidden = (jax.nn.silu(causal_taps(gate_pre, valve_conv_stencil)) * causal_taps(up_pre, widening_conv_stencil)).astype(jnp.bfloat16)
    channel = grouped_sum(hidden.reshape(TOKENS, FFN_UNITS), narrowing_map, N_TP)
    return (first.astype(jnp.float32) + norm_rows(channel, dense_final_norm_gain)).astype(jnp.bfloat16)
```

```python
import functools

import jax
import jax.numpy as jnp
from jax import lax
from jax.experimental import pallas as pl
from jax.experimental.pallas import tpu as pltpu
from jax.sharding import PartitionSpec as P

EPS = 1e-06
STEEPNESS = 16.0
MESH = pl.DeviceIdType.MESH
F32 = jnp.float32
BF16 = jnp.bfloat16
NEG = -1e30


def mm(a, b):
    return jnp.dot(a, b, preferred_element_type=F32)


def mm_nt(a, b):
    return lax.dot_general(a, b, (((1,), (1,)), ((), ())), preferred_element_type=F32)


def split2(v):
    hi = v.astype(BF16)
    return hi, (v - hi.astype(F32)).astype(BF16)


def layer_kernel(
    dims,
    x_hbm, q_hbm, k_hbm, v_hbm, comb_hbm, gate_hbm, up_hbm, down_hbm, exc_hbm,
    g1_ref, gaf_ref, gdi_ref, gdf_ref, egn_ref, left_ref, right_ref, const_ref, tapg_ref, tapu_ref,
    out_ref,
    xb, X, XG, F, wqkv, wc, wgu, wd, exc, ss, hout, hidden, G, firstb, acc, so, si, o2, orr, oll, ih, ifl,
    local_sem, zrecv, zsend, yrecv, ysend, agrecv, agsend, ssrecv, sssend, sibrecv, sibsend, rsrecv, rssend,
):
    NG, NZ, NTP = dims
    T, OC = xb.shape
    D = X.shape[1]
    NX = NTP // 2
    KD = q_hbm.shape[1]
    VD = v_hbm.shape[1]
    FU = gate_hbm.shape[1]
    RZ = q_hbm.shape[0]
    CZ = comb_hbm.shape[1]
    PER = OC // CZ
    H = T // 2
    HALF = NZ // 2

    g, z, t = lax.axis_index("grp"), lax.axis_index("fs"), lax.axis_index("tp")
    par = lax.rem(g, 2)
    pg = g + 1 - 2 * par
    xi, c = t // 2, lax.rem(t, 2)
    chip_r, chip_l, chip_2 = lax.rem(xi + 1, NX), lax.rem(xi + NX - 1, NX), lax.rem(xi + 2, NX)
    sib = 2 * xi + 1 - c
    tr, tl = 2 * chip_r + c, 2 * chip_l + c
    zr, zl = lax.rem(z + 1, NZ), lax.rem(z + NZ - 1, NZ)

    def m(v, n):
        return pl.multiple_of(v, n)

    def wview(ref, o, r0, rows):
        return ref.at[pl.ds(m(o * RZ + r0, 16), rows), :]

    def cview(ref, o, r0, rows):
        return ref.at[o // PER, pl.ds(m(r0, 16), rows), pl.ds(m(lax.rem(o, PER) * CZ, CZ), CZ)]

    def guview(o, r0, rows, c0, cols):
        return wgu.at[pl.ds(m(o * RZ + r0, 16), rows), pl.ds(m(c0, 128), cols)]

    VR = comb_hbm.shape[0]
    b_m, b_c = 80, VR - 160
    c_m = 2 * FU // 3
    d_m = FU // 3
    PHASES = {
        "A": [(lambda o, p, i=i: wview(wqkv, o, p * 48 + 16 * i, 16), True) for i in range(3)]
        + [(lambda o, p, i=i: wview(wqkv, o, 96 + 16 * i, 16), False) for i in range((RZ - 96) // 16)],
        "B": [
            (lambda o, p: cview(wc, o, p * b_m, b_m), True),
            (lambda o, p: cview(wc, o, 2 * b_m, b_c), False),
        ],
        "P": [
            (lambda o, p: guview(o, 0, RZ // 2, p * c_m, c_m), True),
            (lambda o, p: guview(o, 0, RZ // 2, 2 * c_m, c_m), False),
        ],
        "Q": [
            (lambda o, p: guview(o, RZ // 2, RZ // 2, p * c_m, c_m), True),
            (lambda o, p: guview(o, RZ // 2, RZ // 2, 2 * c_m, c_m), False),
        ],
        "D": [
            (lambda o, p: cview(wd, o, p * d_m, d_m), True),
            (lambda o, p: cview(wd, o, 2 * d_m, d_m), False),
        ],
    }
    ANTIPODE = {"A": ((0, 2, 4), (1, 3)), "B": ((0,), (1,)), "P": ((0,), (1,)), "Q": ((1,), (0,)), "D": ((0,), (1,))}
    ZBASE, YBASE, zn, yn = {}, {}, 0, 0
    for name, chunks in PHASES.items():
        ZBASE[name], YBASE[name] = zn, yn
        zn += len(chunks)
        yn += sum(e for _, e in chunks)
    pending_z, pending_y = {}, {}

    def zcopy(phase, ci, d, hop):
        o = lax.rem(z + NZ - hop, NZ) if d == 0 else lax.rem(z + hop, NZ)
        view = PHASES[phase][ci][0](o, par)
        return pltpu.make_async_remote_copy(
            src_ref=view, dst_ref=view,
            send_sem=zsend.at[d, ZBASE[phase] + ci, hop % 2],
            recv_sem=zrecv.at[d, ZBASE[phase] + ci, hop],
            device_id={"fs": zr if d == 0 else zl}, device_id_type=MESH,
        )

    def zstart(phase, ci, d, hop):
        key = (d, ZBASE[phase] + ci, hop % 2)
        if key in pending_z:
            pending_z.pop(key).wait_send()
        copy = zcopy(phase, ci, d, hop)
        copy.start()
        pending_z[key] = copy

    def zwait(phase, ci, d, s):
        o = lax.rem(z + NZ - s, NZ) if d == 0 else lax.rem(z + s, NZ)
        view = PHASES[phase][ci][0](o, par)
        pltpu.make_async_remote_copy(
            src_ref=view, dst_ref=view,
            send_sem=zsend.at[d, ZBASE[phase] + ci, 0],
            recv_sem=zrecv.at[d, ZBASE[phase] + ci, s - 1],
            device_id={"fs": zr if d == 0 else zl}, device_id_type=MESH,
        ).wait_recv()

    def ycopy(phase, ci, d, s, p):
        yi = YBASE[phase] + [i for i, (_, e) in enumerate(PHASES[phase]) if e].index(ci)
        rel = (NZ - s) % NZ if d == 0 else s
        o = lax.rem(z + rel, NZ)
        view = PHASES[phase][ci][0](o, p)
        return yi, pltpu.make_async_remote_copy(
            src_ref=view, dst_ref=view,
            send_sem=ysend.at[yi, d, s % 2],
            recv_sem=yrecv.at[yi, rel],
            device_id={"grp": pg}, device_id_type=MESH,
        )

    def ystart(phase, ci, d, s):
        yi, copy = ycopy(phase, ci, d, s, par)
        key = (yi, d, s % 2)
        if key in pending_y:
            pending_y.pop(key).wait_send()
        copy.start()
        pending_y[key] = copy

    def own_sends(phase):
        for ci in range(len(PHASES[phase])):
            for d in (0, 1):
                zstart(phase, ci, d, 0)

    deferred = []

    def y_flush():
        for args in deferred:
            ystart(*args)
        deferred.clear()

    def tick(phase, s, hold=False):
        for ci, (_, exchanged) in enumerate(PHASES[phase]):
            for d in (0, 1):
                if s == HALF and ci not in ANTIPODE[phase][d]:
                    continue
                zwait(phase, ci, d, s)
                if s < HALF - 1 or (s == HALF - 1 and ci in ANTIPODE[phase][d]):
                    zstart(phase, ci, d, s)
                if exchanged and hold:
                    deferred.append((phase, ci, d, s))
                elif exchanged:
                    ystart(phase, ci, d, s)

    def y_all(phase):
        for s in range(1, HALF + 1):
            for ci, (_, exchanged) in enumerate(PHASES[phase]):
                if exchanged:
                    for d in (0, 1):
                        if s == HALF and ci not in ANTIPODE[phase][d]:
                            continue
                        ycopy(phase, ci, d, s, 1 - par)[1].wait_recv()

    zo = z
    locals_ = [
        (x_hbm, X.at[:, pl.ds(m(t * OC, OC), OC)]),
        (q_hbm, wqkv.at[pl.ds(m(zo * RZ, 16), RZ), 0:KD]),
        (k_hbm, wqkv.at[pl.ds(m(zo * RZ, 16), RZ), KD : 2 * KD]),
        (v_hbm, wqkv.at[pl.ds(m(zo * RZ, 16), RZ), 2 * KD : 2 * KD + VD]),
        (comb_hbm, cview(wc, zo, 0, VR)),
        (gate_hbm, wgu.at[pl.ds(m(zo * RZ, 16), RZ), 0:FU]),
        (up_hbm, wgu.at[pl.ds(m(zo * RZ, 16), RZ), FU : 2 * FU]),
        (down_hbm, cview(wd, zo, 0, FU)),
        (exc_hbm, exc),
        (x_hbm, xb),
    ]
    loads = [pltpu.make_async_copy(a, b, local_sem.at[i]) for i, (a, b) in enumerate(locals_)]
    for copy in loads:
        copy.start()

    barrier = pltpu.get_barrier_semaphore()
    for d in range(1, NTP):
        pl.semaphore_signal(barrier, inc=1, device_id={"tp": lax.rem(t + d, NTP)}, device_id_type=MESH)
    for other in (zr, zl):
        pl.semaphore_signal(barrier, inc=1, device_id={"fs": other}, device_id_type=MESH)
    pl.semaphore_signal(barrier, inc=1, device_id={"grp": pg}, device_id_type=MESH)
    for i in range(0, 4):
        loads[i].wait()
    pl.semaphore_wait(barrier, NTP + 2)
    own_sends("A")

    row_iota = lax.broadcasted_iota(jnp.int32, (T, 1), 0)
    lane_iota = lax.broadcasted_iota(jnp.int32, (128, 128), 1)

    def gain_row(ref):
        per = OC // 128
        rows = [ref[pl.ds(t * per + i, 1), :] for i in range(per)]
        return jnp.concatenate(rows, axis=1)

    pending = []

    NB = T // 128

    def ss_send(k, cols):
        mat = jnp.zeros((128, 128), F32)
        for i, col in enumerate(cols):
            for j in range(NB):
                mat = jnp.where(lane_iota == i * NB + j, col[j * 128 : (j + 1) * 128], mat)
        ss[k, t] = mat.T[0:16, :]
        for d in range(1, NTP):
            copy = pltpu.make_async_remote_copy(
                src_ref=ss.at[k, t], dst_ref=ss.at[k, t],
                send_sem=sssend.at[k, d], recv_sem=ssrecv.at[k, d],
                device_id={"tp": lax.rem(t + d, NTP)}, device_id_type=MESH,
            )
            copy.start()
            pending.append(copy)

    def ss_total(k):
        for d in range(1, NTP):
            src = ss.at[k, lax.rem(t + NTP - d, NTP)]
            pltpu.make_async_remote_copy(
                src_ref=src, dst_ref=src, send_sem=sssend.at[k, d], recv_sem=ssrecv.at[k, d],
                device_id={"tp": lax.rem(t + d, NTP)}, device_id_type=MESH,
            ).wait_recv()
        total = ss[k, 0]
        for i in range(1, NTP):
            total = total + ss[k, i]
        return total

    def columns(rows):
        cols = jnp.concatenate([rows, jnp.zeros((120, 128), F32)], axis=0).T
        pick = lambda a: jnp.concatenate([cols[:, a + j : a + j + 1] for j in range(NB)], axis=0)
        return pick(0), pick(NB)

    def scale_into(ref, lo, hi):
        for l in range(lo, hi):
            cols = slice(l * 128, (l + 1) * 128)
            XG[:, cols] = (X[:, cols].astype(F32) * ref[l : l + 1, :]).astype(BF16)

    def part(buf, o, h):
        return buf.at[pl.ds(h * H, H), pl.ds(m(o * OC, OC), OC)]

    def ag_copy(buf, k, slot, o, h, dev):
        view = part(buf, o, h)
        return pltpu.make_async_remote_copy(
            src_ref=view, dst_ref=view, send_sem=agsend.at[k, slot], recv_sem=agrecv.at[k, slot],
            device_id={"tp": dev}, device_id_type=MESH,
        )

    def ag_start(buf, k):
        for slot, h, dev in ((0, 0, tr), (2, 1, tl), (1, 1, tr), (3, 0, tl), (6, 0, sib), (7, 1, sib)):
            copy = ag_copy(buf, k, slot, t, h, dev)
            copy.start()
            pending.append(copy)

    SRC = {0: (tl, 0), 1: (tl, 1), 2: (tr, 1), 3: (tr, 0), 4: (2 * chip_2 + c, 0), 5: (2 * chip_2 + c, 1)}

    def ag_take(buf, k, slots):
        for slot in slots:
            o, h = SRC[slot]
            ag_copy(buf, k, slot, o, h, sib).wait_recv()
            sends = [(slot + 8, sib)]
            if slot == 0:
                sends = [(4, tr)] + sends
            if slot == 2:
                sends = [(5, tl)] + sends
            for target, dev in sends:
                copy = ag_copy(buf, k, target, o, h, dev)
                copy.start()
                pending.append(copy)

    def ag_end(buf, k):
        for slot in (6, 7):
            ag_copy(buf, k, slot, sib, slot - 6, sib).wait_recv()
        for slot in range(6):
            o, h = SRC[slot]
            ag_copy(buf, k, slot + 8, o, h, sib).wait_recv()

    ag_start(X, 0)
    loads[9].wait()
    x32 = xb[...].astype(F32)
    ss_send(0, [jnp.sum(x32 * x32, axis=1, keepdims=True)])
    for i in range(4, 9):
        loads[i].wait()
    NL = D // 128

    tick("A", 1)
    own_sends("B")
    tick("A", 2)
    ag_take(X, 0, (0, 2))
    tick("A", 3)
    ag_take(X, 0, (1, 3))
    tick("B", 1, True)
    tick("A", 4)
    tick("B", 2, True)
    ag_take(X, 0, (4, 5))
    tick("A", 5)
    tick("B", 3, True)
    ag_end(X, 0)
    tick("A", 6)
    scale_into(g1_ref, 0, NL // 2)
    tick("B", 4, True)
    tick("A", 7)
    scale_into(g1_ref, NL // 2, NL)
    tick("B", 5, True)
    tick("A", 8)
    y_flush()
    tick("B", 6)
    own_sends("P")
    total0 = ss_total(0)
    r1, _ = columns(lax.rsqrt(total0[0:8] / D + EPS))
    y_all("A")

    qk = mm(XG[...], wqkv[:, 0 : 2 * KD]) * r1
    q = qk[:, 0:KD].astype(BF16).astype(F32) * KD ** (-0.5)
    k = qk[:, KD : 2 * KD].astype(BF16).astype(F32)
    v = (mm(XG[...], wqkv[:, 2 * KD : 2 * KD + VD]) * r1).astype(BF16)
    tick("B", 7)
    own_sends("Q")
    low = mm_nt(XG[...], left_ref[...]) * r1
    low_hi, low_lo = split2(low)
    right_hi, right_lo = split2(right_ref[...])
    pre = mm(low_hi, right_hi) + (mm(low_lo, right_hi) + mm(low_hi, right_lo)) + const_ref[...]
    ld = (jnp.minimum(pre, 0.0) - jnp.log1p(jnp.exp(-jnp.abs(pre)))) / STEEPNESS + exc[...]

    ri = lax.broadcasted_iota(jnp.int32, (128, 128), 0)
    tri = jnp.where(ri >= lane_iota, 1.0, 0.0).astype(BF16)
    ld_hi, ld_lo = split2(ld)
    pieces, carry = [], jnp.zeros((1, KD), F32)
    for j in range(T // 128):
        rows = slice(j * 128, (j + 1) * 128)
        run = mm(tri, ld_hi[rows]) + mm(tri, ld_lo[rows]) + carry
        carry = run[127:128]
        pieces.append(run)
    b = jnp.concatenate(pieces, axis=0)
    tick("B", 8)

    def offsets(span):
        b3 = b.reshape(T // span, span, KD)
        return (b3 - b3[:, span // 2 - 1 : span // 2, :]).reshape(T, KD)

    def level(span):
        d = offsets(span)
        second = lax.rem(row_iota, span) >= span // 2
        e = jnp.exp(jnp.where(second, d, -d))
        return jnp.where(second, q * e, 0.0).astype(BF16), jnp.where(second, 0.0, k * e).astype(BF16)

    dd = offsets(32)
    qd, kd = (q * jnp.exp(dd)).astype(BF16), (k * jnp.exp(-dd)).astype(BF16)
    q64, k64 = level(64)
    q128, k128 = level(128)
    q256, k256 = level(256)
    q512, k512 = level(512)
    tick("P", 1)
    ci_ = lane_iota
    in32 = (ri // 32 == ci_ // 32) & (ri >= ci_)
    in64 = (ri // 64 == ci_ // 64) & (ri // 32 != ci_ // 32)
    diag = []
    for j in range(T // 128):
        rows = slice(j * 128, (j + 1) * 128)
        s = jnp.where(in32, mm_nt(qd[rows], kd[rows]), 0.0)
        s = s + jnp.where(in64, mm_nt(q64[rows], k64[rows]), 0.0)
        s = s + mm_nt(q128[rows], k128[rows])
        diag.append(s.astype(BF16))
    zero128 = jnp.zeros((128, 128), BF16)
    halves = []
    for j in range(2):
        lo = slice(j * 256, j * 256 + 128)
        hi = slice(j * 256 + 128, (j + 1) * 256)
        cross = mm_nt(q256[hi], k256[lo]).astype(BF16)
        top = mm(diag[2 * j], v[lo])
        bottom = mm(jnp.concatenate([cross, diag[2 * j + 1]], axis=1), v[j * 256 : (j + 1) * 256])
        halves.append(jnp.concatenate([top, bottom], axis=0))
    far = mm_nt(q512[256:512], k512[0:256]).astype(BF16)
    heads = jnp.concatenate([halves[0], halves[1] + mm(far, v[0:256])], axis=0)
    hs = lax.rsqrt(jnp.mean(heads * heads, axis=1, keepdims=True) + EPS)
    hout[...] = (heads * hs * egn_ref[...]).astype(BF16)
    tick("Q", 1)
    own_sends("D")
    y_all("B")

    def rs(k, lhs_ref, w, between):
        sibs = []
        order = (chip_2, chip_r, chip_l, xi)

        def products(n):
            so[k, n] = mm(lhs_ref[...], w[2 * order[n] + 1 - c]).astype(BF16)
            copy = pltpu.make_async_remote_copy(
                src_ref=so.at[k, n], dst_ref=si.at[k, n], send_sem=sibsend.at[k, n], recv_sem=sibrecv.at[k, n],
                device_id={"tp": sib}, device_id_type=MESH,
            )
            copy.start()
            pending.append(copy)
            sibs.append(copy)
            acc[n] = mm(lhs_ref[...], w[2 * order[n] + c])

        def send(slot, src, dst, dev):
            copy = pltpu.make_async_remote_copy(
                src_ref=src, dst_ref=dst, send_sem=rssend.at[k, slot], recv_sem=rsrecv.at[k, slot],
                device_id={"tp": dev}, device_id_type=MESH,
            )
            copy.start()
            pending.append(copy)

        def take(slot, dst):
            pltpu.make_async_remote_copy(
                src_ref=dst, dst_ref=dst, send_sem=rssend.at[k, slot], recv_sem=rsrecv.at[k, slot],
                device_id={"tp": sib}, device_id_type=MESH,
            ).wait_recv()

        lo, hi = pl.ds(0, H), pl.ds(H, H)
        products(0)
        products(1)
        sibs[0].wait_recv()
        o2[k, lo, :] = (acc[0, lo, :] + si[k, 0, lo, :].astype(F32)).astype(BF16)
        send(0, o2.at[k, lo], ih.at[k, 0], tr)
        o2[k, hi, :] = (acc[0, hi, :] + si[k, 0, hi, :].astype(F32)).astype(BF16)
        send(1, o2.at[k, hi], ih.at[k, 1], tl)
        products(2)
        sibs[1].wait_recv()
        orr[k, hi, :] = (acc[1, hi, :] + si[k, 1, hi, :].astype(F32)).astype(BF16)
        send(2, orr.at[k, hi], ifl.at[k, 0, hi], tr)
        between(0)
        products(3)
        sibs[2].wait_recv()
        oll[k, lo, :] = (acc[2, lo, :] + si[k, 2, lo, :].astype(F32)).astype(BF16)
        send(4, oll.at[k, lo], ifl.at[k, 1, lo], tl)
        between(1)
        take(0, ih.at[k, 0])
        orr[k, lo, :] = (acc[1, lo, :] + si[k, 1, lo, :].astype(F32) + ih[k, 0].astype(F32)).astype(BF16)
        send(3, orr.at[k, lo], ifl.at[k, 0, lo], tr)
        take(1, ih.at[k, 1])
        oll[k, hi, :] = (acc[2, hi, :] + si[k, 2, hi, :].astype(F32) + ih[k, 1].astype(F32)).astype(BF16)
        send(5, oll.at[k, hi], ifl.at[k, 1, hi], tl)
        sibs[3].wait_recv()
        between(2)
        take(2, ifl.at[k, 0, hi])
        take(4, ifl.at[k, 1, lo])
        between(3)
        take(3, ifl.at[k, 0, lo])
        take(5, ifl.at[k, 1, hi])
        return acc[3] + si[k, 3].astype(F32) + (ifl[k, 0].astype(F32) + ifl[k, 1].astype(F32))

    def between0(i):
        if i == 0:
            tick("P", 2)
        elif i == 1:
            tick("Q", 2)
            tick("P", 3)
        elif i == 2:
            tick("Q", 3)
            tick("D", 1)
            scale_into(gdi_ref, 0, NL // 2)
            tick("P", 4)
        else:
            tick("Q", 4)
            scale_into(gdi_ref, NL // 2, NL)

    mixed = rs(0, hout, wc, between0)
    mg = mixed * gain_row(gaf_ref)
    F[:, pl.ds(m(t * OC, OC), OC)] = (mg * gain_row(gdi_ref)).astype(BF16)
    ag_start(F, 1)
    x32 = xb[...].astype(F32)
    ss_send(1, [jnp.sum(a, axis=1, keepdims=True) for a in (mixed * mixed, x32 * mg, mg * mg)])
    acc[3] = mg
    tick("P", 5)
    tick("D", 2)
    tick("Q", 5)
    ag_take(F, 1, (0, 2))
    tick("P", 6)
    tick("D", 3)
    tick("Q", 6)
    ag_take(F, 1, (1, 3))
    tick("P", 7)
    tick("D", 4)
    tick("Q", 7)
    ag_take(F, 1, (4, 5))
    tick("P", 8)
    tick("D", 5)
    tick("Q", 8)
    y_all("P")
    y_all("Q")
    PAD = 8
    G[0:PAD, :] = jnp.zeros((PAD, 2 * FU), F32)
    for n in range(2 * FU // 256):
        cols = slice(n * 256, (n + 1) * 256)
        G[PAD : PAD + T, cols] = mm(XG[...], wgu[:, cols])
    tick("D", 6)
    ag_end(F, 1)
    total1 = ss_total(1)
    ra_rows = lax.rsqrt(total1[0:NB] / D + EPS)
    squares = total0[0:NB] + 2.0 * ra_rows * total1[NB : 2 * NB] + ra_rows * ra_rows * total1[2 * NB : 3 * NB]
    ra, r2 = columns(jnp.concatenate([ra_rows, lax.rsqrt(squares / D + EPS)], axis=0))

    for n in range(2 * FU // 256):
        cols = slice(n * 256, (n + 1) * 256)
        G[PAD : PAD + T, cols] = (G[PAD : PAD + T, cols] + mm(F[...], wgu[:, cols]) * ra) * r2
    tick("D", 7)
    firstb[...] = (xb[...].astype(F32) + acc[3] * ra).astype(BF16)

    def taps(ref, base):
        w = ref[:, base % FU : base % FU + 128].astype(F32)
        n = w.shape[0]
        total = None
        for j in range(n):
            term = w[j : j + 1] * G[PAD - (n - 1) + j : PAD - (n - 1) + j + T, base : base + 128]
            total = term if total is None else total + term
        return total

    for n in range(FU // 128):
        gc, uc = taps(tapg_ref, n * 128), taps(tapu_ref, FU + n * 128)
        hidden[:, n * 128 : (n + 1) * 128] = (gc / (1.0 + jnp.exp(-gc)) * uc).astype(BF16)
    tick("D", 8)
    y_all("D")
    channel = rs(1, hidden, wd, lambda i: None)
    ss_send(3, [jnp.sum(channel * channel, axis=1, keepdims=True)])
    acc[3] = channel
    for copy in list(pending_z.values()) + list(pending_y.values()) + pending[: -(NTP - 1)]:
        copy.wait_send()
    rc, _ = columns(lax.rsqrt(ss_total(3)[0:8] / D + EPS))
    out_ref[...] = (firstb[...].astype(F32) + acc[3] * rc * gain_row(gdf_ref)).astype(BF16)
    for copy in pending[-(NTP - 1) :]:
        copy.wait_send()


def on_device(
    dims, x, g1, egn, gaf, gdi, gdf, wq, wk, wv, left, right, const, excess, comb, gate, up, tapg, tapu, down
):
    NG, NZ, NTP = dims
    T, OC = x.shape
    D = OC * NTP
    KD, VD, FU = wq.shape[1], wv.shape[1], gate.shape[1]
    any_ = pl.BlockSpec(memory_space=pl.ANY)
    vm = pl.BlockSpec(memory_space=pltpu.VMEM)
    DMA = pltpu.SemaphoreType.DMA
    NX = NTP // 2
    VM = pltpu.VMEM
    scratch = [
        VM((T, OC), BF16), VM((T, D), BF16), VM((T, D), BF16), VM((T, D), BF16),
        VM((D, 2 * KD + VD), BF16), VM((NTP, comb.shape[0], OC), BF16), VM((D, 2 * FU), BF16), VM((NTP, FU, OC), BF16),
        VM((T, KD), F32), VM((4, NTP, 16, 128), F32),
        VM((T, VD), BF16), VM((T, FU), BF16), VM((T + 8, 2 * FU), F32), VM((T, OC), BF16),
        VM((NX, T, OC), F32), VM((2, NX, T, OC), BF16), VM((2, NX, T, OC), BF16),
        VM((2, T, OC), BF16), VM((2, T, OC), BF16), VM((2, T, OC), BF16),
        VM((2, 2, T // 2, OC), BF16), VM((2, 2, T, OC), BF16),
        DMA((10,)), DMA((2, 13, NZ // 2)), DMA((2, 13, 2)), DMA((7, NZ)), DMA((7, 2, 2)),
        DMA((2, 14)), DMA((2, 14)), DMA((4, NTP)), DMA((4, NTP)), DMA((2, NX)), DMA((2, NX)), DMA((2, 6)), DMA((2, 6)),
    ]
    return pl.pallas_call(
        functools.partial(layer_kernel, dims),
        out_shape=jax.ShapeDtypeStruct((T, OC), BF16),
        in_specs=[any_] * 9 + [vm] * 10,
        out_specs=vm,
        scratch_shapes=scratch,
        compiler_params=pltpu.CompilerParams(
            collective_id=0, has_side_effects=True, vmem_limit_bytes=60 * 1024 * 1024
        ),
        name="layer",
    )(
        x, wq, wk, wv, comb, gate, up, down, excess,
        g1.reshape(-1, 128), gaf.reshape(-1, 128), gdi.reshape(-1, 128), gdf.reshape(-1, 128),
        egn, left.T, right, const.reshape(1, -1), tapg, tapu,
    )


def solution(mesh):
    dims = (mesh.shape["grp"], mesh.shape["fs"], mesh.shape["tp"])
    placed = (
        P(("grp", "fs"), "tp"), P(), P("tp", None), P(), P(), P(), P("fs", "tp"), P("fs", "tp"), P("fs", "tp"), P(),
        P(None, "tp"), P("tp"), P(("grp", "fs"), "tp"), P("tp", "fs"), P("fs", "tp"), P("fs", "tp"), P(None, "tp"),
        P(None, "tp"), P("tp", "fs"),
    )
    return jax.shard_map(
        functools.partial(on_device, dims), mesh=mesh, in_specs=placed, out_specs=P(("grp", "fs"), "tp"),
        check_vma=False,
    )
```

```python
import functools

import jax
import jax.numpy as jnp
from jax import lax
from jax.experimental import pallas as pl
from jax.experimental.pallas import tpu as pltpu
from jax.sharding import PartitionSpec as P

EPS = 1e-06
STEEPNESS = 16.0
MESH = pl.DeviceIdType.MESH
F32 = jnp.float32
BF16 = jnp.bfloat16
NEG = -1e30


def mm(a, b):
    return jnp.dot(a, b, preferred_element_type=F32)


def mm_nt(a, b):
    return lax.dot_general(a, b, (((1,), (1,)), ((), ())), preferred_element_type=F32)


def split2(v):
    hi = v.astype(BF16)
    return hi, (v - hi.astype(F32)).astype(BF16)


def layer_kernel(
    dims,
    x_hbm, q_hbm, k_hbm, v_hbm, comb_hbm, gate_hbm, up_hbm, down_hbm, exc_hbm,
    g1_ref, gaf_ref, gdi_ref, gdf_ref, egn_ref, left_ref, right_ref, const_ref, tapg_ref, tapu_ref,
    out_ref,
    back, xb, X, XG, F, wqkv, wc, wgu, wd, exc, ss, hout, hidden, G, firstb, acc, so, si, o2, orr, oll, ih, ifl,
    local_sem, zrecv, zsend, yrecv, ysend, agrecv, agsend, ssrecv, sssend, sibrecv, sibsend, rsrecv, rssend,
):
    NG, NZ, NTP = dims
    T, OC = xb.shape
    D = X.shape[1]
    NX = NTP // 2
    KD = q_hbm.shape[1]
    VD = v_hbm.shape[1]
    FU = gate_hbm.shape[1]
    RZ = q_hbm.shape[0]
    CZ = comb_hbm.shape[1]
    PER = OC // CZ
    H = T // 2
    HALF = NZ // 2

    g, z, t = lax.axis_index("grp"), lax.axis_index("fs"), lax.axis_index("tp")
    par = lax.rem(g, 2)
    pg = g + 1 - 2 * par
    xi, c = t // 2, lax.rem(t, 2)
    chip_r, chip_l, chip_2 = lax.rem(xi + 1, NX), lax.rem(xi + NX - 1, NX), lax.rem(xi + 2, NX)
    sib = 2 * xi + 1 - c
    tr, tl = 2 * chip_r + c, 2 * chip_l + c
    zr, zl = lax.rem(z + 1, NZ), lax.rem(z + NZ - 1, NZ)

    def m(v, n):
        return pl.multiple_of(v, n)

    def wview(ref, o, r0, rows):
        return ref.at[pl.ds(m(o * RZ + r0, 16), rows), :]

    def cview(ref, o, r0, rows):
        return ref.at[o // PER, pl.ds(m(r0, 16), rows), pl.ds(m(lax.rem(o, PER) * CZ, CZ), CZ)]

    def guview(o, r0, rows, c0, cols):
        return wgu.at[pl.ds(m(o * RZ + r0, 16), rows), pl.ds(m(c0, 128), cols)]

    VR = comb_hbm.shape[0]
    b_m, b_c = 80, VR - 160
    c_m = 2 * FU // 3
    d_m = FU // 3
    W = 2 * KD + VD
    PHASES = {
        "A": [(lambda o, p, i=i: wview(wqkv, o, p * 48 + 16 * i, 16), True, 16 * W) for i in range(3)]
        + [(lambda o, p, i=i: wview(wqkv, o, 96 + 16 * i, 16), False, 16 * W) for i in range((RZ - 96) // 16)],
        "B": [
            (lambda o, p: cview(wc, o, p * b_m, b_m), True, b_m * CZ),
            (lambda o, p: cview(wc, o, 2 * b_m, b_c), False, b_c * CZ),
        ],
        "P": [
            (lambda o, p: guview(o, 0, RZ // 2, p * c_m, c_m), True, RZ // 2 * c_m),
            (lambda o, p: guview(o, 0, RZ // 2, 2 * c_m, c_m), False, RZ // 2 * c_m),
        ],
        "Q": [
            (lambda o, p: guview(o, RZ // 2, RZ // 2, p * c_m, c_m), True, RZ // 2 * c_m),
            (lambda o, p: guview(o, RZ // 2, RZ // 2, 2 * c_m, c_m), False, RZ // 2 * c_m),
        ],
        "D": [
            (lambda o, p: cview(wd, o, p * d_m, d_m), True, d_m * CZ),
            (lambda o, p: cview(wd, o, 2 * d_m, d_m), False, d_m * CZ),
        ],
    }
    ANTIPODE = {"A": ((0, 2, 4), (1, 3)), "B": ((0,), (1,)), "P": ((0,), (1,)), "Q": ((1,), (0,)), "D": ((0,), (1,))}
    NAMES = list(PHASES)
    ZBASE, zn = {}, 0
    for name, chunks in PHASES.items():
        ZBASE[name] = zn
        zn += len(chunks)

    def block(elements):
        if elements % (16 * W) == 0:
            return wqkv.at[0 : elements // W, :]
        return wqkv.at[0 : elements // 128, 0:128]

    def arrived(sem, view):
        pltpu.make_async_remote_copy(
            src_ref=view, dst_ref=view, send_sem=sem, recv_sem=sem, device_id={"tp": sib}, device_id_type=MESH
        ).wait_recv()

    def left(sem, view):
        pltpu.make_async_remote_copy(
            src_ref=view, dst_ref=view, send_sem=sem, recv_sem=sem, device_id={"tp": sib}, device_id_type=MESH
        ).wait_send()

    sent_z = {(d, n): 0 for d in (0, 1) for n in NAMES}
    sent_y = {n: 0 for n in NAMES}

    def steps_from(d, s):
        return lax.rem(z + NZ - s, NZ) if d == 0 else lax.rem(z + s, NZ)

    def zstart(phase, ci, d, hop):
        view = PHASES[phase][ci][0](steps_from(d, hop), par)
        pltpu.make_async_remote_copy(
            src_ref=view, dst_ref=view,
            send_sem=zsend.at[d, NAMES.index(phase)], recv_sem=zrecv.at[ZBASE[phase] + ci, hop],
            device_id={"fs": zr if d == 0 else zl}, device_id_type=MESH,
        ).start()
        sent_z[d, phase] += PHASES[phase][ci][2]

    def ystart(phase, ci, d, s):
        view = PHASES[phase][ci][0](steps_from(d, s), par)
        i = NAMES.index(phase)
        pltpu.make_async_remote_copy(
            src_ref=view, dst_ref=view, send_sem=ysend.at[i], recv_sem=yrecv.at[i],
            device_id={"grp": pg}, device_id_type=MESH,
        ).start()
        sent_y[phase] += PHASES[phase][ci][2]

    def own_sends(phase):
        for ci in range(len(PHASES[phase])):
            for d in (0, 1):
                zstart(phase, ci, d, 0)

    deferred = []

    def y_flush():
        for args in deferred:
            ystart(*args)
        deferred.clear()

    def tick(phase, s, hold=False):
        for ci, (_, exchanged, elements) in enumerate(PHASES[phase]):
            dirs = [d for d in (0, 1) if s < HALF or ci in ANTIPODE[phase][d]]
            arrived(zrecv.at[ZBASE[phase] + ci, s - 1], block(elements * len(dirs)))
            for d in dirs:
                if s < HALF - 1 or (s == HALF - 1 and ci in ANTIPODE[phase][d]):
                    zstart(phase, ci, d, s)
            for d in dirs:
                if exchanged and hold:
                    deferred.append((phase, ci, d, s))
                elif exchanged:
                    ystart(phase, ci, d, s)

    def y_all(phase):
        arrived(yrecv.at[NAMES.index(phase)], block(sum(n for _, e, n in PHASES[phase] if e) * (NZ - 1)))

    zo = z
    locals_ = [
        (x_hbm, X.at[:, pl.ds(m(t * OC, OC), OC)]),
        (q_hbm, wqkv.at[pl.ds(m(zo * RZ, 16), RZ), 0:KD]),
        (k_hbm, wqkv.at[pl.ds(m(zo * RZ, 16), RZ), KD : 2 * KD]),
        (v_hbm, wqkv.at[pl.ds(m(zo * RZ, 16), RZ), 2 * KD : 2 * KD + VD]),
        (comb_hbm, cview(wc, zo, 0, VR)),
        (gate_hbm, wgu.at[pl.ds(m(zo * RZ, 16), RZ), 0:FU]),
        (up_hbm, wgu.at[pl.ds(m(zo * RZ, 16), RZ), FU : 2 * FU]),
        (down_hbm, cview(wd, zo, 0, FU)),
        (exc_hbm, exc),
        (x_hbm, xb),
    ]
    loads = [pltpu.make_async_copy(a, b, local_sem.at[i]) for i, (a, b) in enumerate(locals_)]
    for copy in loads:
        copy.start()

    back[...] = jnp.zeros_like(back)

    barrier = pltpu.get_barrier_semaphore()
    for d in range(1, NTP):
        pl.semaphore_signal(barrier, inc=1, device_id={"tp": lax.rem(t + d, NTP)}, device_id_type=MESH)
    for other in (zr, zl):
        pl.semaphore_signal(barrier, inc=1, device_id={"fs": other}, device_id_type=MESH)
    pl.semaphore_signal(barrier, inc=1, device_id={"grp": pg}, device_id_type=MESH)
    for i in range(0, 4):
        loads[i].wait()
    pl.semaphore_wait(barrier, NTP + 2)
    own_sends("A")

    row_iota = lax.broadcasted_iota(jnp.int32, (T, 1), 0)
    lane_iota = lax.broadcasted_iota(jnp.int32, (128, 128), 1)

    def gain_row(ref):
        per = OC // 128
        rows = [ref[pl.ds(t * per + i, 1), :] for i in range(per)]
        return jnp.concatenate(rows, axis=1)

    NB = T // 128

    def ss_store(k, cols):
        mat = jnp.zeros((128, 128), F32)
        for i, col in enumerate(cols):
            for j in range(NB):
                mat = jnp.where(lane_iota == i * NB + j, col[j * 128 : (j + 1) * 128], mat)
        ss[k, t] = mat.T[0:16, :]

    def settle(block_):
        rows = 16 if block_.dtype == BF16 else 8
        got = block_.reshape(-1, rows, block_.shape[-1])
        back[...] = back[...] + jnp.max(got, axis=0)[0:8, 0:128].astype(F32)

    def ss_start(k):
        settle(ss[k, t])
        for d in range(1, NTP):
            pltpu.make_async_remote_copy(
                src_ref=ss.at[k, t], dst_ref=ss.at[k, t], send_sem=sssend.at[k], recv_sem=ssrecv.at[k],
                device_id={"tp": lax.rem(t + d, NTP)}, device_id_type=MESH,
            ).start()

    def ss_total(k):
        arrived(ssrecv.at[k], ss.at[k, 0 : NTP - 1])
        total = ss[k, 0]
        for i in range(1, NTP):
            total = total + ss[k, i]
        return total

    def columns(rows):
        cols = jnp.concatenate([rows, jnp.zeros((120, 128), F32)], axis=0).T
        pick = lambda a: jnp.concatenate([cols[:, a + j : a + j + 1] for j in range(NB)], axis=0)
        return pick(0), pick(NB)

    def scale_into(scale, ref, lo, hi):
        for l in range(lo, hi):
            cols = slice(l * 128, (l + 1) * 128)
            XG[:, cols] = (X[:, cols].astype(F32) * scale * ref[l : l + 1, :]).astype(BF16)

    def part(buf, o, h):
        return buf.at[pl.ds(h * H, H), pl.ds(m(o * OC, OC), OC)]

    AG_SEM = (0, 1, 2, 3, 4, 5, 6, 6, 7, 8, 7, 8, 9, 9)

    def ag_send(buf, k, slot, o, h, dev):
        view = part(buf, o, h)
        pltpu.make_async_remote_copy(
            src_ref=view, dst_ref=view, send_sem=agsend.at[k], recv_sem=agrecv.at[k, AG_SEM[slot]],
            device_id={"tp": dev}, device_id_type=MESH,
        ).start()

    def ag_start(buf, k):
        for slot, h, dev in ((0, 0, tr), (2, 1, tl), (1, 1, tr), (3, 0, tl), (6, 0, sib), (7, 1, sib)):
            ag_send(buf, k, slot, t, h, dev)

    SRC = {0: (tl, 0), 1: (tl, 1), 2: (tr, 1), 3: (tr, 0), 4: (2 * chip_2 + c, 0), 5: (2 * chip_2 + c, 1)}

    def ag_take(buf, k, slots):
        for slot in slots:
            o, h = SRC[slot]
            arrived(agrecv.at[k, AG_SEM[slot]], part(buf, o, h))
            if slot == 0:
                ag_send(buf, k, 4, o, h, tr)
            if slot == 2:
                ag_send(buf, k, 5, o, h, tl)
            ag_send(buf, k, slot + 8, o, h, sib)

    SIB_SRC = {6: (sib, 0), 7: (sib, 1)}
    SIB_SRC.update({slot + 8: (o + 1 - 2 * c, h) for slot, (o, h) in SRC.items()})

    def ag_end(buf, k, pairs=((6, 7), (8, 10), (9, 11), (12, 13)), then=lambda o, h: None):
        for pair in pairs:
            arrived(agrecv.at[k, AG_SEM[pair[0]]], buf.at[:, 0:OC])
            for slot in pair:
                then(*SIB_SRC[slot])

    ag_start(X, 0)
    loads[9].wait()
    x32 = xb[...].astype(F32)
    ss_store(0, [jnp.sum(x32 * x32, axis=1, keepdims=True)])
    for i in range(4, 9):
        loads[i].wait()
    NL = D // 128

    tick("A", 1)
    ss_start(0)
    own_sends("B")
    tick("A", 2)
    ag_take(X, 0, (0, 2))
    tick("A", 3)
    ag_take(X, 0, (1, 3))
    tick("B", 1, True)
    tick("A", 4)
    tick("B", 2, True)
    ag_take(X, 0, (4, 5))
    tick("A", 5)
    tick("B", 3, True)
    ag_end(X, 0)
    total0 = ss_total(0)
    r1, _ = columns(lax.rsqrt(total0[0:8] / D + EPS))
    tick("A", 6)
    scale_into(r1, g1_ref, 0, NL // 2)
    tick("B", 4, True)
    tick("A", 7)
    scale_into(r1, g1_ref, NL // 2, NL)
    tick("B", 5, True)
    tick("A", 8)
    y_flush()
    tick("B", 6)
    y_all("A")
    own_sends("P")

    qk = mm(XG[...], wqkv[:, 0 : 2 * KD])
    q = qk[:, 0:KD].astype(BF16).astype(F32) * KD ** (-0.5)
    k = qk[:, KD : 2 * KD].astype(BF16).astype(F32)
    v = mm(XG[...], wqkv[:, 2 * KD : 2 * KD + VD]).astype(BF16)
    tick("B", 7)
    own_sends("Q")
    low = mm_nt(XG[...], left_ref[...])
    low_hi, low_lo = split2(low)
    right_hi, right_lo = split2(right_ref[...])
    pre = mm(low_hi, right_hi) + (mm(low_lo, right_hi) + mm(low_hi, right_lo)) + const_ref[...]
    ld = (jnp.minimum(pre, 0.0) - jnp.log1p(jnp.exp(-jnp.abs(pre)))) / STEEPNESS + exc[...]

    ri = lax.broadcasted_iota(jnp.int32, (128, 128), 0)
    tri = jnp.where(ri >= lane_iota, 1.0, 0.0).astype(BF16)
    ld_hi, ld_lo = split2(ld)
    pieces, carry = [], jnp.zeros((1, KD), F32)
    for j in range(T // 128):
        rows = slice(j * 128, (j + 1) * 128)
        run = mm(tri, ld_hi[rows]) + mm(tri, ld_lo[rows]) + carry
        carry = run[127:128]
        pieces.append(run)
    b = jnp.concatenate(pieces, axis=0)
    tick("B", 8)
    own_sends("D")

    def offsets(span):
        b3 = b.reshape(T // span, span, KD)
        return (b3 - b3[:, span // 2 - 1 : span // 2, :]).reshape(T, KD)

    def level(span):
        d = offsets(span)
        second = lax.rem(row_iota, span) >= span // 2
        e = jnp.exp(jnp.where(second, d, -d))
        return jnp.where(second, q * e, 0.0).astype(BF16), jnp.where(second, 0.0, k * e).astype(BF16)

    dd = offsets(32)
    qd_hi, qd_lo = split2(q * jnp.exp(dd))
    kd_hi, kd_lo = split2(k * jnp.exp(-dd))
    qd = jnp.concatenate([qd_hi, qd_lo, qd_hi], axis=1)
    kd = jnp.concatenate([kd_hi, kd_hi, kd_lo], axis=1)
    q64, k64 = level(64)
    q128, k128 = level(128)
    q256, k256 = level(256)
    q512, k512 = level(512)
    tick("P", 1)
    ci_ = lane_iota
    in32 = (ri // 32 == ci_ // 32) & (ri >= ci_)
    in64 = (ri // 64 == ci_ // 64) & (ri // 32 != ci_ // 32)
    diag = []
    for j in range(T // 128):
        rows = slice(j * 128, (j + 1) * 128)
        s = jnp.where(in32, mm_nt(qd[rows], kd[rows]), 0.0)
        s = s + jnp.where(in64, mm_nt(q64[rows], k64[rows]), 0.0)
        s = s + mm_nt(q128[rows], k128[rows])
        diag.append(s.astype(BF16))
    zero128 = jnp.zeros((128, 128), BF16)
    halves = []
    for j in range(2):
        lo = slice(j * 256, j * 256 + 128)
        hi = slice(j * 256 + 128, (j + 1) * 256)
        cross = mm_nt(q256[hi], k256[lo]).astype(BF16)
        top = mm(diag[2 * j], v[lo])
        bottom = mm(jnp.concatenate([cross, diag[2 * j + 1]], axis=1), v[j * 256 : (j + 1) * 256])
        halves.append(jnp.concatenate([top, bottom], axis=0))
    far = mm_nt(q512[256:512], k512[0:256]).astype(BF16)
    heads = jnp.concatenate([halves[0], halves[1] + mm(far, v[0:256])], axis=0)
    hs = lax.rsqrt(jnp.mean(heads * heads, axis=1, keepdims=True) + EPS)
    hout[...] = (heads * hs * egn_ref[...]).astype(BF16)
    tick("Q", 1)
    y_all("B")

    def rs(k, lhs_ref, w, between):
        order = (chip_2, chip_r, chip_l, xi)

        def products(n):
            so[k, n] = mm(lhs_ref[...], w[2 * order[n] + 1 - c]).astype(BF16)
            acc[n] = mm(lhs_ref[...], w[2 * order[n] + c])
            pltpu.make_async_remote_copy(
                src_ref=so.at[k, n], dst_ref=si.at[k, n], send_sem=sibsend.at[k], recv_sem=sibrecv.at[k, n],
                device_id={"tp": sib}, device_id_type=MESH,
            ).start()

        def send(sem, src, dst, dev):
            pltpu.make_async_remote_copy(
                src_ref=src, dst_ref=dst, send_sem=rssend.at[k], recv_sem=rsrecv.at[k, sem],
                device_id={"tp": dev}, device_id_type=MESH,
            ).start()

        def with_sib(n, rows):
            return acc[n, rows, :] + si[k, n, rows, :].astype(F32)

        lo, hi = pl.ds(0, H), pl.ds(H, H)
        products(0)
        products(1)
        between(0)
        arrived(sibrecv.at[k, 0], si.at[k, 0])
        o2[k, lo, :] = with_sib(0, lo).astype(BF16)
        o2[k, hi, :] = with_sib(0, hi).astype(BF16)
        settle(o2[k, hi, :])
        send(0, o2.at[k, lo], ih.at[k, 0], tr)
        send(1, o2.at[k, hi], ih.at[k, 1], tl)
        between(1)
        products(2)
        arrived(sibrecv.at[k, 1], si.at[k, 1])
        orr[k, hi, :] = with_sib(1, hi).astype(BF16)
        between(2)
        products(3)
        send(2, orr.at[k, hi], ifl.at[k, 0, hi], tr)
        arrived(sibrecv.at[k, 2], si.at[k, 2])
        oll[k, lo, :] = with_sib(2, lo).astype(BF16)
        acc[1, lo, :] = with_sib(1, lo)
        acc[2, hi, :] = with_sib(2, hi)
        settle(oll[k, lo, :])
        send(2, oll.at[k, lo], ifl.at[k, 1, lo], tl)
        between(3)
        arrived(rsrecv.at[k, 0], ih.at[k, 0])
        orr[k, lo, :] = (acc[1, lo, :] + ih[k, 0].astype(F32)).astype(BF16)
        arrived(rsrecv.at[k, 1], ih.at[k, 1])
        oll[k, hi, :] = (acc[2, hi, :] + ih[k, 1].astype(F32)).astype(BF16)
        settle(orr[k, lo, :])
        send(3, orr.at[k, lo], ifl.at[k, 0, lo], tr)
        arrived(sibrecv.at[k, 3], si.at[k, 3])
        settle(oll[k, hi, :])
        send(3, oll.at[k, hi], ifl.at[k, 1, hi], tl)
        acc[3] = acc[3] + si[k, 3].astype(F32)
        between(4)
        arrived(rsrecv.at[k, 2], ifl.at[k, 0])
        between(5)
        arrived(rsrecv.at[k, 3], ifl.at[k, 0])
        return acc[3] + (ifl[k, 0].astype(F32) + ifl[k, 1].astype(F32))

    WORK = (("P2",), ("Q2",), ("D1",), ("P3", "Q3"), ("D2", "P4", "Q4"), ("D3", "P5"))

    def ticks(*names):
        for name in names:
            tick(name[0], int(name[1]))

    def between0(i):
        ticks(*WORK[i])

    mixed = rs(0, hout, wc, between0)
    mg = mixed * gain_row(gaf_ref)
    F[:, pl.ds(m(t * OC, OC), OC)] = mg.astype(BF16)
    x32 = xb[...].astype(F32)
    ss_store(1, [jnp.sum(a, axis=1, keepdims=True) for a in (mixed * mixed, x32 * mg, mg * mg)])
    settle(F[H:T, pl.ds(m(t * OC, OC), OC)])
    ag_start(F, 1)
    acc[3] = mg
    ss_start(1)
    ticks("Q5", "D4", "P6")
    total1 = ss_total(1)
    ra_rows = lax.rsqrt(total1[0:NB] / D + EPS)
    squares = total0[0:NB] + 2.0 * ra_rows * total1[NB : 2 * NB] + ra_rows * ra_rows * total1[2 * NB : 3 * NB]
    ra, r2 = columns(jnp.concatenate([ra_rows, lax.rsqrt(squares / D + EPS)], axis=0))
    firstb[...] = (x32 + acc[3] * ra).astype(BF16)

    def join(o, h):
        rows, cols = pl.ds(h * H, H), pl.ds(m(o * OC, OC), OC)
        gain = jnp.concatenate([gdi_ref[pl.ds(o * (OC // 128) + i, 1), :] for i in range(OC // 128)], axis=1)
        whole = X[rows, cols].astype(F32) + F[rows, cols].astype(F32) * ra[h * H : (h + 1) * H]
        XG[rows, cols] = (whole * gain).astype(BF16)

    join(t, 0)
    join(t, 1)
    ticks("Q6", "D5")
    ag_take(F, 1, (0, 2))
    join(*SRC[0])
    join(*SRC[2])
    ag_end(F, 1, ((6, 7),), join)
    ticks("P7", "Q7", "D6")
    ag_take(F, 1, (1, 3))
    join(*SRC[1])
    join(*SRC[3])
    ag_end(F, 1, ((8, 10),), join)
    ticks("P8", "Q8", "D7")
    ag_take(F, 1, (4, 5))
    join(*SRC[4])
    join(*SRC[5])
    ag_end(F, 1, ((9, 11),), join)
    ticks("D8")
    y_all("P")
    y_all("Q")
    ag_end(F, 1, ((12, 13),), join)

    PAD = 8
    G[0:PAD, :] = jnp.zeros((PAD, 2 * FU), F32)
    for n in range(2 * FU // 256):
        cols = slice(n * 256, (n + 1) * 256)
        G[PAD : PAD + T, cols] = mm(XG[...], wgu[:, cols]) * r2

    def taps(ref, base):
        w = ref[:, base % FU : base % FU + 128].astype(F32)
        n = w.shape[0]
        total = None
        for j in range(n):
            term = w[j : j + 1] * G[PAD - (n - 1) + j : PAD - (n - 1) + j + T, base : base + 128]
            total = term if total is None else total + term
        return total

    for n in range(FU // 128):
        gc, uc = taps(tapg_ref, n * 128), taps(tapu_ref, FU + n * 128)
        hidden[:, n * 128 : (n + 1) * 128] = (gc / (1.0 + jnp.exp(-gc)) * uc).astype(BF16)
    y_all("D")
    channel = rs(1, hidden, wd, lambda i: None)
    ss_store(2, [jnp.sum(channel * channel, axis=1, keepdims=True)])
    acc[3] = channel
    ss_start(2)
    for i, name in enumerate(NAMES):
        for d in (0, 1):
            left(zsend.at[d, i], block(sent_z[d, name]))
        left(ysend.at[i], block(sent_y[name]))
    for k in (0, 1):
        left(agsend.at[k], X.at[0 : 14 * H * OC // D, :])
        left(sibsend.at[k], so.at[k])
        left(rssend.at[k], X.at[0 : 6 * H * OC // D, :])
        left(sssend.at[k], ss.at[k, 0 : NTP - 1])
    rc, _ = columns(lax.rsqrt(ss_total(2)[0:8] / D + EPS))
    out_ref[...] = (firstb[...].astype(F32) + acc[3] * rc * gain_row(gdf_ref)).astype(BF16)
    left(sssend.at[2], ss.at[2, 0 : NTP - 1])


def on_device(
    dims, x, g1, egn, gaf, gdi, gdf, wq, wk, wv, left, right, const, excess, comb, gate, up, tapg, tapu, down
):
    NG, NZ, NTP = dims
    T, OC = x.shape
    D = OC * NTP
    KD, VD, FU = wq.shape[1], wv.shape[1], gate.shape[1]
    any_ = pl.BlockSpec(memory_space=pl.ANY)
    vm = pl.BlockSpec(memory_space=pltpu.VMEM)
    DMA = pltpu.SemaphoreType.DMA
    NX = NTP // 2
    VM = pltpu.VMEM
    scratch = [
        VM((8, 128), F32), VM((T, OC), BF16), VM((T, D), BF16), VM((T, D), BF16), VM((T, D), BF16),
        VM((D, 2 * KD + VD), BF16), VM((NTP, comb.shape[0], OC), BF16), VM((D, 2 * FU), BF16), VM((NTP, FU, OC), BF16),
        VM((T, KD), F32), VM((3, NTP, 16, 128), F32),
        VM((T, VD), BF16), VM((T, FU), BF16), VM((T + 8, 2 * FU), F32), VM((T, OC), BF16),
        VM((NX, T, OC), F32), VM((2, NX, T, OC), BF16), VM((2, NX, T, OC), BF16),
        VM((2, T, OC), BF16), VM((2, T, OC), BF16), VM((2, T, OC), BF16),
        VM((2, 2, T // 2, OC), BF16), VM((2, 2, T, OC), BF16),
        DMA((10,)), DMA((13, NZ // 2)), DMA((2, 5)), DMA((5,)), DMA((5,)),
        DMA((2, 10)), DMA((2,)), DMA((3,)), DMA((3,)), DMA((2, NX)), DMA((2,)), DMA((2, 4)), DMA((2,)),
    ]
    return pl.pallas_call(
        functools.partial(layer_kernel, dims),
        out_shape=jax.ShapeDtypeStruct((T, OC), BF16),
        in_specs=[any_] * 9 + [vm] * 10,
        out_specs=vm,
        scratch_shapes=scratch,
        compiler_params=pltpu.CompilerParams(
            collective_id=0, has_side_effects=True, vmem_limit_bytes=60 * 1024 * 1024
        ),
        name="layer",
    )(
        x, wq, wk, wv, comb, gate, up, down, excess,
        g1.reshape(-1, 128), gaf.reshape(-1, 128), gdi.reshape(-1, 128), gdf.reshape(-1, 128),
        egn, left.T, right, const.reshape(1, -1), tapg, tapu,
    )


def solution(mesh):
    dims = (mesh.shape["grp"], mesh.shape["fs"], mesh.shape["tp"])
    placed = (
        P(("grp", "fs"), "tp"), P(), P("tp", None), P(), P(), P(), P("fs", "tp"), P("fs", "tp"), P("fs", "tp"), P(),
        P(None, "tp"), P("tp"), P(("grp", "fs"), "tp"), P("tp", "fs"), P("fs", "tp"), P("fs", "tp"), P(None, "tp"),
        P(None, "tp"), P("tp", "fs"),
    )
    return jax.shard_map(
        functools.partial(on_device, dims), mesh=mesh, in_specs=placed, out_specs=P(("grp", "fs"), "tp"),
        check_vma=False,
    )
```

```python
import functools

import jax
import jax.numpy as jnp
from jax import lax
from jax.experimental import pallas as pl
from jax.experimental.pallas import tpu as pltpu
from jax.sharding import PartitionSpec as P

EPS = 1e-06
STEEPNESS = 16.0
MESH = pl.DeviceIdType.MESH
F32 = jnp.float32
BF16 = jnp.bfloat16
NEG = -1e30


def mm(a, b):
    return jnp.dot(a, b, preferred_element_type=F32)


def mm_nt(a, b):
    return lax.dot_general(a, b, (((1,), (1,)), ((), ())), preferred_element_type=F32)


def split2(v):
    hi = v.astype(BF16)
    return hi, (v - hi.astype(F32)).astype(BF16)


def layer_kernel(
    dims,
    x_hbm, q_hbm, k_hbm, v_hbm, comb_hbm, gate_hbm, up_hbm, down_hbm, exc_hbm,
    g1_ref, gaf_ref, gdi_ref, gdf_ref, egn_ref, left_ref, right_ref, const_ref, tapg_ref, tapu_ref,
    out_ref,
    back, xb, X, XG, F, wqkv, wc, wgu, wd, exc, ss, hout, hidden, G, firstb, acc, so, si, o2, orr, oll, ih, ifl,
    local_sem, zrecv, zsend, yrecv, ysend, agrecv, agsend, ssrecv, sssend, sibrecv, sibsend, rsrecv, rssend,
):
    NG, NZ, NTP = dims
    T, OC = xb.shape
    D = X.shape[1]
    NX = NTP // 2
    KD = q_hbm.shape[1]
    VD = v_hbm.shape[1]
    FU = gate_hbm.shape[1]
    RZ = q_hbm.shape[0]
    CZ = comb_hbm.shape[1]
    PER = OC // CZ
    H = T // 2
    HALF = NZ // 2

    g, z, t = lax.axis_index("grp"), lax.axis_index("fs"), lax.axis_index("tp")
    par = lax.rem(g, 2)
    pg = g + 1 - 2 * par
    xi, c = t // 2, lax.rem(t, 2)
    chip_r, chip_l, chip_2 = lax.rem(xi + 1, NX), lax.rem(xi + NX - 1, NX), lax.rem(xi + 2, NX)
    sib = 2 * xi + 1 - c
    tr, tl = 2 * chip_r + c, 2 * chip_l + c
    zr, zl = lax.rem(z + 1, NZ), lax.rem(z + NZ - 1, NZ)

    def m(v, n):
        return pl.multiple_of(v, n)

    def wview(ref, o, r0, rows):
        return ref.at[pl.ds(m(o * RZ + r0, 16), rows), :]

    def cview(ref, o, r0, rows):
        return ref.at[o // PER, pl.ds(m(r0, 16), rows), pl.ds(m(lax.rem(o, PER) * CZ, CZ), CZ)]

    def guview(o, r0, rows, c0, cols):
        return wgu.at[pl.ds(m(o * RZ + r0, 16), rows), pl.ds(m(c0, 128), cols)]

    VR = comb_hbm.shape[0]
    b_m, b_c = 80, VR - 160
    c_m = 2 * FU // 3
    d_m = FU // 3
    W = 2 * KD + VD
    PHASES = {
        "A": [(lambda o, p, i=i: wview(wqkv, o, p * 48 + 16 * i, 16), True, 16 * W) for i in range(3)]
        + [(lambda o, p, i=i: wview(wqkv, o, 96 + 16 * i, 16), False, 16 * W) for i in range((RZ - 96) // 16)],
        "B": [
            (lambda o, p: cview(wc, o, p * b_m, b_m), True, b_m * CZ),
            (lambda o, p: cview(wc, o, 2 * b_m, b_c), False, b_c * CZ),
        ],
        "P": [
            (lambda o, p: guview(o, 0, RZ // 2, p * c_m, c_m), True, RZ // 2 * c_m),
            (lambda o, p: guview(o, 0, RZ // 2, 2 * c_m, c_m), False, RZ // 2 * c_m),
        ],
        "Q": [
            (lambda o, p: guview(o, RZ // 2, RZ // 2, p * c_m, c_m), True, RZ // 2 * c_m),
            (lambda o, p: guview(o, RZ // 2, RZ // 2, 2 * c_m, c_m), False, RZ // 2 * c_m),
        ],
        "D": [
            (lambda o, p: cview(wd, o, p * d_m, d_m), True, d_m * CZ),
            (lambda o, p: cview(wd, o, 2 * d_m, d_m), False, d_m * CZ),
        ],
    }
    ANTIPODE = {"A": ((0, 2, 4), (1, 3)), "B": ((0,), (1,)), "P": ((0,), (1,)), "Q": ((1,), (0,)), "D": ((0,), (1,))}
    NAMES = list(PHASES)
    ZBASE, zn = {}, 0
    for name, chunks in PHASES.items():
        ZBASE[name] = zn
        zn += len(chunks)

    def block(elements):
        if elements % (16 * W) == 0:
            return wqkv.at[0 : elements // W, :]
        return wqkv.at[0 : elements // 128, 0:128]

    def arrived(sem, view):
        pltpu.make_async_remote_copy(
            src_ref=view, dst_ref=view, send_sem=sem, recv_sem=sem, device_id={"tp": sib}, device_id_type=MESH
        ).wait_recv()

    def left(sem, view):
        pltpu.make_async_remote_copy(
            src_ref=view, dst_ref=view, send_sem=sem, recv_sem=sem, device_id={"tp": sib}, device_id_type=MESH
        ).wait_send()

    sent_z = {(d, n): 0 for d in (0, 1) for n in NAMES}
    sent_y = {n: 0 for n in NAMES}

    def steps_from(d, s):
        return lax.rem(z + NZ - s, NZ) if d == 0 else lax.rem(z + s, NZ)

    def zstart(phase, ci, d, hop):
        view = PHASES[phase][ci][0](steps_from(d, hop), par)
        pltpu.make_async_remote_copy(
            src_ref=view, dst_ref=view,
            send_sem=zsend.at[d, NAMES.index(phase)], recv_sem=zrecv.at[ZBASE[phase] + ci, hop],
            device_id={"fs": zr if d == 0 else zl}, device_id_type=MESH,
        ).start()
        sent_z[d, phase] += PHASES[phase][ci][2]

    def ystart(phase, ci, d, s):
        view = PHASES[phase][ci][0](steps_from(d, s), par)
        i = NAMES.index(phase)
        pltpu.make_async_remote_copy(
            src_ref=view, dst_ref=view, send_sem=ysend.at[i], recv_sem=yrecv.at[i],
            device_id={"grp": pg}, device_id_type=MESH,
        ).start()
        sent_y[phase] += PHASES[phase][ci][2]

    def own_sends(phase):
        for ci in range(len(PHASES[phase])):
            for d in (0, 1):
                zstart(phase, ci, d, 0)

    deferred = []

    def y_flush():
        for args in deferred:
            ystart(*args)
        deferred.clear()

    def tick(phase, s, hold=False):
        for ci, (_, exchanged, elements) in enumerate(PHASES[phase]):
            dirs = [d for d in (0, 1) if s < HALF or ci in ANTIPODE[phase][d]]
            arrived(zrecv.at[ZBASE[phase] + ci, s - 1], block(elements * len(dirs)))
            for d in dirs:
                if s < HALF - 1 or (s == HALF - 1 and ci in ANTIPODE[phase][d]):
                    zstart(phase, ci, d, s)
            for d in dirs:
                if exchanged and hold:
                    deferred.append((phase, ci, d, s))
                elif exchanged:
                    ystart(phase, ci, d, s)

    def y_all(phase):
        arrived(yrecv.at[NAMES.index(phase)], block(sum(n for _, e, n in PHASES[phase] if e) * (NZ - 1)))

    zo = z
    locals_ = [
        (x_hbm, X.at[:, pl.ds(m(t * OC, OC), OC)]),
        (q_hbm, wqkv.at[pl.ds(m(zo * RZ, 16), RZ), 0:KD]),
        (k_hbm, wqkv.at[pl.ds(m(zo * RZ, 16), RZ), KD : 2 * KD]),
        (v_hbm, wqkv.at[pl.ds(m(zo * RZ, 16), RZ), 2 * KD : 2 * KD + VD]),
        (comb_hbm, cview(wc, zo, 0, VR)),
        (gate_hbm, wgu.at[pl.ds(m(zo * RZ, 16), RZ), 0:FU]),
        (up_hbm, wgu.at[pl.ds(m(zo * RZ, 16), RZ), FU : 2 * FU]),
        (down_hbm, cview(wd, zo, 0, FU)),
        (exc_hbm, exc),
        (x_hbm, xb),
    ]
    loads = [pltpu.make_async_copy(a, b, local_sem.at[i]) for i, (a, b) in enumerate(locals_)]
    for copy in loads:
        copy.start()

    back[...] = jnp.zeros_like(back)

    barrier = pltpu.get_barrier_semaphore()
    for d in range(1, NTP):
        pl.semaphore_signal(barrier, inc=1, device_id={"tp": lax.rem(t + d, NTP)}, device_id_type=MESH)
    for other in (zr, zl):
        pl.semaphore_signal(barrier, inc=1, device_id={"fs": other}, device_id_type=MESH)
    pl.semaphore_signal(barrier, inc=1, device_id={"grp": pg}, device_id_type=MESH)
    for i in range(0, 4):
        loads[i].wait()
    pl.semaphore_wait(barrier, NTP + 2)
    own_sends("A")

    row_iota = lax.broadcasted_iota(jnp.int32, (T, 1), 0)
    lane_iota = lax.broadcasted_iota(jnp.int32, (128, 128), 1)

    def gain_row(ref):
        per = OC // 128
        rows = [ref[pl.ds(t * per + i, 1), :] for i in range(per)]
        return jnp.concatenate(rows, axis=1)

    NB = T // 128

    def ss_store(k, cols):
        mat = jnp.zeros((128, 128), F32)
        for i, col in enumerate(cols):
            for j in range(NB):
                mat = jnp.where(lane_iota == i * NB + j, col[j * 128 : (j + 1) * 128], mat)
        ss[k, t] = mat.T[0:16, :]

    def settle(block_):
        rows = 16 if block_.dtype == BF16 else 8
        got = block_.reshape(-1, rows, block_.shape[-1])
        back[...] = back[...] + jnp.max(got, axis=0)[0:8, 0:128].astype(F32)

    def ss_start(k):
        settle(ss[k, t])
        for d in range(1, NTP):
            pltpu.make_async_remote_copy(
                src_ref=ss.at[k, t], dst_ref=ss.at[k, t], send_sem=sssend.at[k], recv_sem=ssrecv.at[k],
                device_id={"tp": lax.rem(t + d, NTP)}, device_id_type=MESH,
            ).start()

    def ss_total(k):
        arrived(ssrecv.at[k], ss.at[k, 0 : NTP - 1])
        total = ss[k, 0]
        for i in range(1, NTP):
            total = total + ss[k, i]
        return total

    def columns(rows):
        cols = jnp.concatenate([rows, jnp.zeros((120, 128), F32)], axis=0).T
        pick = lambda a: jnp.concatenate([cols[:, a + j : a + j + 1] for j in range(NB)], axis=0)
        return pick(0), pick(NB)

    def scale_into(scale, ref, lo, hi):
        for l in range(lo, hi):
            cols = slice(l * 128, (l + 1) * 128)
            XG[:, cols] = (X[:, cols].astype(F32) * scale * ref[l : l + 1, :]).astype(BF16)

    def part(buf, o, h):
        return buf.at[pl.ds(h * H, H), pl.ds(m(o * OC, OC), OC)]

    AG_SEM = (0, 1, 2, 3, 4, 5, 6, 6, 7, 8, 7, 8, 9, 9)

    def ag_send(buf, k, slot, o, h, dev):
        view = part(buf, o, h)
        pltpu.make_async_remote_copy(
            src_ref=view, dst_ref=view, send_sem=agsend.at[k], recv_sem=agrecv.at[k, AG_SEM[slot]],
            device_id={"tp": dev}, device_id_type=MESH,
        ).start()

    def ag_start(buf, k):
        for slot, h, dev in ((0, 0, tr), (2, 1, tl), (1, 1, tr), (3, 0, tl), (6, 0, sib), (7, 1, sib)):
            ag_send(buf, k, slot, t, h, dev)

    SRC = {0: (tl, 0), 1: (tl, 1), 2: (tr, 1), 3: (tr, 0), 4: (2 * chip_2 + c, 0), 5: (2 * chip_2 + c, 1)}

    def ag_take(buf, k, slots):
        for slot in slots:
            o, h = SRC[slot]
            arrived(agrecv.at[k, AG_SEM[slot]], part(buf, o, h))
            if slot == 0:
                ag_send(buf, k, 4, o, h, tr)
            if slot == 2:
                ag_send(buf, k, 5, o, h, tl)
            ag_send(buf, k, slot + 8, o, h, sib)

    SIB_SRC = {6: (sib, 0), 7: (sib, 1)}
    SIB_SRC.update({slot + 8: (o + 1 - 2 * c, h) for slot, (o, h) in SRC.items()})

    def ag_end(buf, k, pairs=((6, 7), (8, 10), (9, 11), (12, 13)), then=lambda o, h: None):
        for pair in pairs:
            arrived(agrecv.at[k, AG_SEM[pair[0]]], buf.at[:, 0:OC])
            for slot in pair:
                then(*SIB_SRC[slot])

    ag_start(X, 0)
    loads[9].wait()
    x32 = xb[...].astype(F32)
    ss_store(0, [jnp.sum(x32 * x32, axis=1, keepdims=True)])
    for i in range(4, 9):
        loads[i].wait()
    NL = D // 128

    tick("A", 1)
    ss_start(0)
    own_sends("B")
    tick("A", 2)
    ag_take(X, 0, (0, 2))
    tick("A", 3)
    ag_take(X, 0, (1, 3))
    tick("B", 1, True)
    tick("A", 4)
    tick("B", 2, True)
    ag_take(X, 0, (4, 5))
    tick("A", 5)
    tick("B", 3, True)
    ag_end(X, 0)
    total0 = ss_total(0)
    r1, _ = columns(lax.rsqrt(total0[0:8] / D + EPS))
    tick("A", 6)
    scale_into(r1, g1_ref, 0, NL // 2)
    tick("B", 4, True)
    tick("A", 7)
    scale_into(r1, g1_ref, NL // 2, NL)
    tick("B", 5, True)
    tick("A", 8)
    y_flush()
    tick("B", 6)
    y_all("A")
    own_sends("P")

    qk = mm(XG[...], wqkv[:, 0 : 2 * KD])
    q = qk[:, 0:KD].astype(BF16).astype(F32) * KD ** (-0.5)
    k = qk[:, KD : 2 * KD].astype(BF16).astype(F32)
    v = mm(XG[...], wqkv[:, 2 * KD : 2 * KD + VD]).astype(BF16)
    tick("B", 7)
    own_sends("Q")
    low = mm_nt(XG[...], left_ref[...])
    low_hi, low_lo = split2(low)
    right_hi, right_lo = split2(right_ref[...])
    pre = mm(low_hi, right_hi) + (mm(low_lo, right_hi) + mm(low_hi, right_lo)) + const_ref[...]
    ld = (jnp.minimum(pre, 0.0) - jnp.log1p(jnp.exp(-jnp.abs(pre)))) / STEEPNESS + exc[...]

    ri = lax.broadcasted_iota(jnp.int32, (128, 128), 0)
    tri = jnp.where(ri >= lane_iota, 1.0, 0.0).astype(BF16)
    ld_hi, ld_lo = split2(ld)
    pieces, carry = [], jnp.zeros((1, KD), F32)
    for j in range(T // 128):
        rows = slice(j * 128, (j + 1) * 128)
        run = mm(tri, ld_hi[rows]) + mm(tri, ld_lo[rows]) + carry
        carry = run[127:128]
        pieces.append(run)
    b = jnp.concatenate(pieces, axis=0)
    tick("B", 8)
    tick("P", 1)
    own_sends("D")

    def offsets(span):
        b3 = b.reshape(T // span, span, KD)
        return (b3 - b3[:, span // 2 - 1 : span // 2, :]).reshape(T, KD)

    def level(span):
        d = offsets(span)
        second = lax.rem(row_iota, span) >= span // 2
        e = jnp.exp(jnp.where(second, d, -d))
        return jnp.where(second, q * e, 0.0).astype(BF16), jnp.where(second, 0.0, k * e).astype(BF16)

    dd = offsets(32)
    qd_hi, qd_lo = split2(q * jnp.exp(dd))
    kd_hi, kd_lo = split2(k * jnp.exp(-dd))
    qd = jnp.concatenate([qd_hi, qd_lo, qd_hi], axis=1)
    kd = jnp.concatenate([kd_hi, kd_hi, kd_lo], axis=1)
    q64, k64 = level(64)
    q128, k128 = level(128)
    q256, k256 = level(256)
    q512, k512 = level(512)
    tick("Q", 1)
    ci_ = lane_iota
    in32 = (ri // 32 == ci_ // 32) & (ri >= ci_)
    in64 = (ri // 64 == ci_ // 64) & (ri // 32 != ci_ // 32)
    diag = []
    for j in range(T // 128):
        rows = slice(j * 128, (j + 1) * 128)
        s = jnp.where(in32, mm_nt(qd[rows], kd[rows]), 0.0)
        s = s + jnp.where(in64, mm_nt(q64[rows], k64[rows]), 0.0)
        s = s + mm_nt(q128[rows], k128[rows])
        diag.append(s.astype(BF16))
    zero128 = jnp.zeros((128, 128), BF16)
    halves = []
    for j in range(2):
        lo = slice(j * 256, j * 256 + 128)
        hi = slice(j * 256 + 128, (j + 1) * 256)
        cross = mm_nt(q256[hi], k256[lo]).astype(BF16)
        top = mm(diag[2 * j], v[lo])
        bottom = mm(jnp.concatenate([cross, diag[2 * j + 1]], axis=1), v[j * 256 : (j + 1) * 256])
        halves.append(jnp.concatenate([top, bottom], axis=0))
    far = mm_nt(q512[256:512], k512[0:256]).astype(BF16)
    heads = jnp.concatenate([halves[0], halves[1] + mm(far, v[0:256])], axis=0)
    hs = lax.rsqrt(jnp.mean(heads * heads, axis=1, keepdims=True) + EPS)
    hout[...] = (heads * hs * egn_ref[...]).astype(BF16)
    tick("P", 2)
    y_all("B")

    def rs(k, lhs_ref, w, between):
        order = (chip_2, chip_r, chip_l, xi)

        def products(n):
            so[k, n] = mm(lhs_ref[...], w[2 * order[n] + 1 - c]).astype(BF16)
            acc[n] = mm(lhs_ref[...], w[2 * order[n] + c])
            pltpu.make_async_remote_copy(
                src_ref=so.at[k, n], dst_ref=si.at[k, n], send_sem=sibsend.at[k], recv_sem=sibrecv.at[k, n],
                device_id={"tp": sib}, device_id_type=MESH,
            ).start()

        def send(sem, src, dst, dev):
            pltpu.make_async_remote_copy(
                src_ref=src, dst_ref=dst, send_sem=rssend.at[k], recv_sem=rsrecv.at[k, sem],
                device_id={"tp": dev}, device_id_type=MESH,
            ).start()

        def with_sib(n, rows):
            return acc[n, rows, :] + si[k, n, rows, :].astype(F32)

        lo, hi = pl.ds(0, H), pl.ds(H, H)
        products(0)
        products(1)
        between(0)
        arrived(sibrecv.at[k, 0], si.at[k, 0])
        o2[k, lo, :] = with_sib(0, lo).astype(BF16)
        o2[k, hi, :] = with_sib(0, hi).astype(BF16)
        settle(o2[k, hi, :])
        send(0, o2.at[k, lo], ih.at[k, 0], tr)
        send(1, o2.at[k, hi], ih.at[k, 1], tl)
        between(1)
        products(2)
        arrived(sibrecv.at[k, 1], si.at[k, 1])
        orr[k, hi, :] = with_sib(1, hi).astype(BF16)
        between(2)
        products(3)
        send(2, orr.at[k, hi], ifl.at[k, 0, hi], tr)
        arrived(sibrecv.at[k, 2], si.at[k, 2])
        oll[k, lo, :] = with_sib(2, lo).astype(BF16)
        acc[1, lo, :] = with_sib(1, lo)
        acc[2, hi, :] = with_sib(2, hi)
        settle(oll[k, lo, :])
        send(2, oll.at[k, lo], ifl.at[k, 1, lo], tl)
        between(3)
        arrived(rsrecv.at[k, 0], ih.at[k, 0])
        orr[k, lo, :] = (acc[1, lo, :] + ih[k, 0].astype(F32)).astype(BF16)
        arrived(rsrecv.at[k, 1], ih.at[k, 1])
        oll[k, hi, :] = (acc[2, hi, :] + ih[k, 1].astype(F32)).astype(BF16)
        settle(orr[k, lo, :])
        send(3, orr.at[k, lo], ifl.at[k, 0, lo], tr)
        arrived(sibrecv.at[k, 3], si.at[k, 3])
        settle(oll[k, hi, :])
        send(3, oll.at[k, hi], ifl.at[k, 1, hi], tl)
        acc[3] = acc[3] + si[k, 3].astype(F32)
        between(4)
        arrived(rsrecv.at[k, 2], ifl.at[k, 0])
        between(5)
        arrived(rsrecv.at[k, 3], ifl.at[k, 0])
        return acc[3] + (ifl[k, 0].astype(F32) + ifl[k, 1].astype(F32))

    WORK = (("Q2",), ("D1",), ("P3",), ("Q3", "P4"), ("D2", "Q4"), ("P5", "D3"))

    def ticks(*names):
        for name in names:
            tick(name[0], int(name[1]))

    def between0(i):
        ticks(*WORK[i])

    mixed = rs(0, hout, wc, between0)
    mg = mixed * gain_row(gaf_ref)
    F[:, pl.ds(m(t * OC, OC), OC)] = mg.astype(BF16)
    x32 = xb[...].astype(F32)
    ss_store(1, [jnp.sum(a, axis=1, keepdims=True) for a in (mixed * mixed, x32 * mg, mg * mg)])
    ss_start(1)
    settle(F[H:T, pl.ds(m(t * OC, OC), OC)])
    ag_start(F, 1)
    acc[3] = mg
    ticks("Q5", "P6", "D4")
    ag_take(F, 1, (0, 2))
    ticks("Q6")
    total1 = ss_total(1)
    ra_rows = lax.rsqrt(total1[0:NB] / D + EPS)
    squares = total0[0:NB] + 2.0 * ra_rows * total1[NB : 2 * NB] + ra_rows * ra_rows * total1[2 * NB : 3 * NB]
    ra, r2 = columns(jnp.concatenate([ra_rows, lax.rsqrt(squares / D + EPS)], axis=0))
    firstb[...] = (x32 + acc[3] * ra).astype(BF16)

    def join(o, h):
        rows, cols = pl.ds(h * H, H), pl.ds(m(o * OC, OC), OC)
        gain = jnp.concatenate([gdi_ref[pl.ds(o * (OC // 128) + i, 1), :] for i in range(OC // 128)], axis=1)
        whole = X[rows, cols].astype(F32) + F[rows, cols].astype(F32) * ra[h * H : (h + 1) * H]
        XG[rows, cols] = (whole * gain).astype(BF16)

    join(t, 0)
    join(t, 1)
    join(*SRC[0])
    join(*SRC[2])
    ag_end(F, 1, ((6, 7),), join)
    ticks("P7", "D5")
    ag_take(F, 1, (1, 3))
    ticks("Q7")
    join(*SRC[1])
    join(*SRC[3])
    ag_end(F, 1, ((8, 10),), join)
    ticks("P8", "D6")
    ag_take(F, 1, (4, 5))
    ticks("Q8")
    join(*SRC[4])
    join(*SRC[5])
    ag_end(F, 1, ((9, 11),), join)
    ag_end(F, 1, ((12, 13),), join)
    ticks("D7")
    y_all("P")
    y_all("Q")

    PAD = 8
    G[0:PAD, :] = jnp.zeros((PAD, 2 * FU), F32)
    for n in range(2 * FU // 256):
        cols = slice(n * 256, (n + 1) * 256)
        G[PAD : PAD + T, cols] = mm(XG[...], wgu[:, cols]) * r2
        if n == 1:
            tick("D", 8)

    def taps(ref, base):
        w = ref[:, base % FU : base % FU + 128].astype(F32)
        n = w.shape[0]
        total = None
        for j in range(n):
            term = w[j : j + 1] * G[PAD - (n - 1) + j : PAD - (n - 1) + j + T, base : base + 128]
            total = term if total is None else total + term
        return total

    for n in range(FU // 128):
        gc, uc = taps(tapg_ref, n * 128), taps(tapu_ref, FU + n * 128)
        hidden[:, n * 128 : (n + 1) * 128] = (gc / (1.0 + jnp.exp(-gc)) * uc).astype(BF16)
    y_all("D")
    channel = rs(1, hidden, wd, lambda i: None)
    ss_store(2, [jnp.sum(channel * channel, axis=1, keepdims=True)])
    acc[3] = channel
    ss_start(2)
    for i, name in enumerate(NAMES):
        for d in (0, 1):
            left(zsend.at[d, i], block(sent_z[d, name]))
        left(ysend.at[i], block(sent_y[name]))
    for k in (0, 1):
        left(agsend.at[k], X.at[0 : 14 * H * OC // D, :])
        left(sibsend.at[k], so.at[k])
        left(rssend.at[k], X.at[0 : 6 * H * OC // D, :])
        left(sssend.at[k], ss.at[k, 0 : NTP - 1])
    rc, _ = columns(lax.rsqrt(ss_total(2)[0:8] / D + EPS))
    out_ref[...] = (firstb[...].astype(F32) + acc[3] * rc * gain_row(gdf_ref)).astype(BF16)
    left(sssend.at[2], ss.at[2, 0 : NTP - 1])


def on_device(
    dims, x, g1, egn, gaf, gdi, gdf, wq, wk, wv, left, right, const, excess, comb, gate, up, tapg, tapu, down
):
    NG, NZ, NTP = dims
    T, OC = x.shape
    D = OC * NTP
    KD, VD, FU = wq.shape[1], wv.shape[1], gate.shape[1]
    any_ = pl.BlockSpec(memory_space=pl.ANY)
    vm = pl.BlockSpec(memory_space=pltpu.VMEM)
    DMA = pltpu.SemaphoreType.DMA
    NX = NTP // 2
    VM = pltpu.VMEM
    scratch = [
        VM((8, 128), F32), VM((T, OC), BF16), VM((T, D), BF16), VM((T, D), BF16), VM((T, D), BF16),
        VM((D, 2 * KD + VD), BF16), VM((NTP, comb.shape[0], OC), BF16), VM((D, 2 * FU), BF16), VM((NTP, FU, OC), BF16),
        VM((T, KD), F32), VM((3, NTP, 16, 128), F32),
        VM((T, VD), BF16), VM((T, FU), BF16), VM((T + 8, 2 * FU), F32), VM((T, OC), BF16),
        VM((NX, T, OC), F32), VM((2, NX, T, OC), BF16), VM((2, NX, T, OC), BF16),
        VM((2, T, OC), BF16), VM((2, T, OC), BF16), VM((2, T, OC), BF16),
        VM((2, 2, T // 2, OC), BF16), VM((2, 2, T, OC), BF16),
        DMA((10,)), DMA((13, NZ // 2)), DMA((2, 5)), DMA((5,)), DMA((5,)),
        DMA((2, 10)), DMA((2,)), DMA((3,)), DMA((3,)), DMA((2, NX)), DMA((2,)), DMA((2, 4)), DMA((2,)),
    ]
    return pl.pallas_call(
        functools.partial(layer_kernel, dims),
        out_shape=jax.ShapeDtypeStruct((T, OC), BF16),
        in_specs=[any_] * 9 + [vm] * 10,
        out_specs=vm,
        scratch_shapes=scratch,
        compiler_params=pltpu.CompilerParams(
            collective_id=0, has_side_effects=True, vmem_limit_bytes=60 * 1024 * 1024
        ),
        name="layer",
    )(
        x, wq, wk, wv, comb, gate, up, down, excess,
        g1.reshape(-1, 128), gaf.reshape(-1, 128), gdi.reshape(-1, 128), gdf.reshape(-1, 128),
        egn, left.T, right, const.reshape(1, -1), tapg, tapu,
    )


def solution(mesh):
    dims = (mesh.shape["grp"], mesh.shape["fs"], mesh.shape["tp"])
    placed = (
        P(("grp", "fs"), "tp"), P(), P("tp", None), P(), P(), P(), P("fs", "tp"), P("fs", "tp"), P("fs", "tp"), P(),
        P(None, "tp"), P("tp"), P(("grp", "fs"), "tp"), P("tp", "fs"), P("fs", "tp"), P("fs", "tp"), P(None, "tp"),
        P(None, "tp"), P("tp", "fs"),
    )
    return jax.shard_map(
        functools.partial(on_device, dims), mesh=mesh, in_specs=placed, out_specs=P(("grp", "fs"), "tp"),
        check_vma=False,
    )
```

```python
import functools

import jax
import jax.numpy as jnp
from jax import lax
from jax.experimental import pallas as pl
from jax.experimental.pallas import tpu as pltpu
from jax.sharding import PartitionSpec as P

EPS = 1e-06
STEEPNESS = 16.0
MESH = pl.DeviceIdType.MESH
F32 = jnp.float32
BF16 = jnp.bfloat16
NEG = -1e30


def mm(a, b):
    return jnp.dot(a, b, preferred_element_type=F32)


def mm_nt(a, b):
    return lax.dot_general(a, b, (((1,), (1,)), ((), ())), preferred_element_type=F32)


def split2(v):
    hi = v.astype(BF16)
    return hi, (v - hi.astype(F32)).astype(BF16)


def layer_kernel(
    dims,
    x_hbm, q_hbm, k_hbm, v_hbm, comb_hbm, gate_hbm, up_hbm, down_hbm, exc_hbm,
    g1_ref, gaf_ref, gdi_ref, gdf_ref, egn_ref, left_ref, right_ref, const_ref, tapg_ref, tapu_ref,
    out_ref,
    back, xb, X, XG, F, wqkv, wc, wgu, wd, exc, ss, hout, hidden, G, firstb, acc, so, si, o2, orr, oll, ih, ifl,
    local_sem, zrecv, zsend, yrecv, ysend, agrecv, agsend, ssrecv, sssend, sibrecv, sibsend, rsrecv, rssend,
):
    NG, NZ, NTP = dims
    T, OC = xb.shape
    D = X.shape[1]
    NX = NTP // 2
    KD = q_hbm.shape[1]
    VD = v_hbm.shape[1]
    FU = gate_hbm.shape[1]
    RZ = q_hbm.shape[0]
    CZ = comb_hbm.shape[1]
    PER = OC // CZ
    H = T // 2
    HALF = NZ // 2

    g, z, t = lax.axis_index("grp"), lax.axis_index("fs"), lax.axis_index("tp")
    par = lax.rem(g, 2)
    pg = g + 1 - 2 * par
    xi, c = t // 2, lax.rem(t, 2)
    chip_r, chip_l, chip_2 = lax.rem(xi + 1, NX), lax.rem(xi + NX - 1, NX), lax.rem(xi + 2, NX)
    sib = 2 * xi + 1 - c
    tr, tl = 2 * chip_r + c, 2 * chip_l + c
    zr, zl = lax.rem(z + 1, NZ), lax.rem(z + NZ - 1, NZ)

    def m(v, n):
        return pl.multiple_of(v, n)

    def wview(ref, o, r0, rows):
        return ref.at[pl.ds(m(o * RZ + r0, 16), rows), :]

    def cview(ref, o, r0, rows):
        return ref.at[o // PER, pl.ds(m(r0, 16), rows), pl.ds(m(lax.rem(o, PER) * CZ, CZ), CZ)]

    VR = comb_hbm.shape[0]
    b_m, b_c = 96, VR - 192
    d_m, d_c = 144, FU - 288
    W = 2 * KD + VD
    PHASES = {
        "A": [(lambda o, p, i=i: wview(wqkv, o, p * 48 + 16 * i, 16), True, 16 * W) for i in range(3)]
        + [(lambda o, p, i=i: wview(wqkv, o, 96 + 16 * i, 16), False, 16 * W) for i in range((RZ - 96) // 16)],
        "B": [
            (lambda o, p: cview(wc, o, p * b_m, b_m), True, b_m * CZ),
            (lambda o, p: cview(wc, o, 2 * b_m, b_c), False, b_c * CZ),
        ],
        "P": [(lambda o, p, i=i: wview(wgu, o, p * 48 + 16 * i, 16), True, 16 * 2 * FU) for i in range(3)],
        "Q": [(lambda o, p, i=i: wview(wgu, o, 96 + 16 * i, 16), False, 16 * 2 * FU) for i in range((RZ - 96) // 16)],
        "D": [
            (lambda o, p: cview(wd, o, p * d_m, d_m), True, d_m * CZ),
            (lambda o, p: cview(wd, o, 2 * d_m, d_c), False, d_c * CZ),
        ],
    }
    ANTIPODE = {"A": ((0, 2, 4), (1, 3)), "B": ((0,), (1,)), "P": ((0,), (1, 2)), "Q": ((0,), (1,)), "D": ((0,), (1,))}
    NAMES = list(PHASES)
    ZBASE, zn = {}, 0
    for name, chunks in PHASES.items():
        ZBASE[name] = zn
        zn += len(chunks)

    def block(elements):
        for ref, wide in ((wgu, 2 * FU), (wqkv, W), (wgu, FU), (wqkv, 128)):
            rows = elements // wide
            if elements % (16 * wide) == 0 and rows <= D:
                return ref.at[0:rows, 0:wide]
        raise ValueError(elements)

    def arrived(sem, view):
        pltpu.make_async_remote_copy(
            src_ref=view, dst_ref=view, send_sem=sem, recv_sem=sem, device_id={"tp": sib}, device_id_type=MESH
        ).wait_recv()

    def left(sem, view):
        pltpu.make_async_remote_copy(
            src_ref=view, dst_ref=view, send_sem=sem, recv_sem=sem, device_id={"tp": sib}, device_id_type=MESH
        ).wait_send()

    sent_z = {(d, n): 0 for d in (0, 1) for n in NAMES}
    sent_y = {n: 0 for n in NAMES}

    def steps_from(d, s):
        return lax.rem(z + NZ - s, NZ) if d == 0 else lax.rem(z + s, NZ)

    def zstart(phase, ci, d, hop):
        view = PHASES[phase][ci][0](steps_from(d, hop), par)
        pltpu.make_async_remote_copy(
            src_ref=view, dst_ref=view,
            send_sem=zsend.at[d, NAMES.index(phase)], recv_sem=zrecv.at[ZBASE[phase] + ci, hop],
            device_id={"fs": zr if d == 0 else zl}, device_id_type=MESH,
        ).start()
        sent_z[d, phase] += PHASES[phase][ci][2]

    def ystart(phase, ci, d, s):
        view = PHASES[phase][ci][0](steps_from(d, s), par)
        i = NAMES.index(phase)
        pltpu.make_async_remote_copy(
            src_ref=view, dst_ref=view, send_sem=ysend.at[i], recv_sem=yrecv.at[i],
            device_id={"grp": pg}, device_id_type=MESH,
        ).start()
        sent_y[phase] += PHASES[phase][ci][2]

    def own_sends(phase):
        for ci in range(len(PHASES[phase])):
            for d in (0, 1):
                zstart(phase, ci, d, 0)

    deferred = []

    def y_flush():
        for args in deferred:
            ystart(*args)
        deferred.clear()

    def tick(phase, s, hold=False):
        for ci, (_, exchanged, elements) in enumerate(PHASES[phase]):
            dirs = [d for d in (0, 1) if s < HALF or ci in ANTIPODE[phase][d]]
            arrived(zrecv.at[ZBASE[phase] + ci, s - 1], block(elements * len(dirs)))
            for d in dirs:
                if s < HALF - 1 or (s == HALF - 1 and ci in ANTIPODE[phase][d]):
                    zstart(phase, ci, d, s)
            for d in dirs:
                if exchanged and hold:
                    deferred.append((phase, ci, d, s))
                elif exchanged:
                    ystart(phase, ci, d, s)

    def y_all(phase):
        arrived(yrecv.at[NAMES.index(phase)], block(sum(n for _, e, n in PHASES[phase] if e) * (NZ - 1)))

    zo = z
    locals_ = [
        (x_hbm, X.at[:, pl.ds(m(t * OC, OC), OC)]),
        (q_hbm, wqkv.at[pl.ds(m(zo * RZ, 16), RZ), 0:KD]),
        (k_hbm, wqkv.at[pl.ds(m(zo * RZ, 16), RZ), KD : 2 * KD]),
        (v_hbm, wqkv.at[pl.ds(m(zo * RZ, 16), RZ), 2 * KD : 2 * KD + VD]),
        (comb_hbm, cview(wc, zo, 0, VR)),
        (gate_hbm, wgu.at[pl.ds(m(zo * RZ, 16), RZ), 0:FU]),
        (up_hbm, wgu.at[pl.ds(m(zo * RZ, 16), RZ), FU : 2 * FU]),
        (down_hbm, cview(wd, zo, 0, FU)),
        (exc_hbm, exc),
        (x_hbm, xb),
    ]
    loads = [pltpu.make_async_copy(a, b, local_sem.at[i]) for i, (a, b) in enumerate(locals_)]
    for copy in loads:
        copy.start()

    back[...] = jnp.zeros_like(back)

    barrier = pltpu.get_barrier_semaphore()
    for d in range(1, NTP):
        pl.semaphore_signal(barrier, inc=1, device_id={"tp": lax.rem(t + d, NTP)}, device_id_type=MESH)
    for other in (zr, zl):
        pl.semaphore_signal(barrier, inc=1, device_id={"fs": other}, device_id_type=MESH)
    pl.semaphore_signal(barrier, inc=1, device_id={"grp": pg}, device_id_type=MESH)
    for i in range(0, 4):
        loads[i].wait()
    pl.semaphore_wait(barrier, NTP + 2)
    own_sends("A")

    row_iota = lax.broadcasted_iota(jnp.int32, (T, 1), 0)
    lane_iota = lax.broadcasted_iota(jnp.int32, (128, 128), 1)

    def gain_row(ref):
        per = OC // 128
        rows = [ref[pl.ds(t * per + i, 1), :] for i in range(per)]
        return jnp.concatenate(rows, axis=1)

    NB = T // 128

    def ss_store(k, cols):
        mat = jnp.zeros((128, 128), F32)
        for i, col in enumerate(cols):
            for j in range(NB):
                mat = jnp.where(lane_iota == i * NB + j, col[j * 128 : (j + 1) * 128], mat)
        ss[k, t] = mat.T[0:16, :]

    def settle(block_):
        rows = 16 if block_.dtype == BF16 else 8
        got = block_.reshape(-1, rows, block_.shape[-1])
        back[...] = back[...] + jnp.max(got, axis=0)[0:8, 0:128].astype(F32)

    def ss_start(k):
        settle(ss[k, t])
        for d in range(1, NTP):
            pltpu.make_async_remote_copy(
                src_ref=ss.at[k, t], dst_ref=ss.at[k, t], send_sem=sssend.at[k], recv_sem=ssrecv.at[k],
                device_id={"tp": lax.rem(t + d, NTP)}, device_id_type=MESH,
            ).start()

    def ss_total(k):
        arrived(ssrecv.at[k], ss.at[k, 0 : NTP - 1])
        total = ss[k, 0]
        for i in range(1, NTP):
            total = total + ss[k, i]
        return total

    def columns(rows):
        cols = jnp.concatenate([rows, jnp.zeros((120, 128), F32)], axis=0).T
        pick = lambda a: jnp.concatenate([cols[:, a + j : a + j + 1] for j in range(NB)], axis=0)
        return pick(0), pick(NB)

    def scale_into(scale, ref, lo, hi):
        for l in range(lo, hi):
            cols = slice(l * 128, (l + 1) * 128)
            XG[:, cols] = (X[:, cols].astype(F32) * scale * ref[l : l + 1, :]).astype(BF16)

    def part(buf, o, h):
        return buf.at[pl.ds(h * H, H), pl.ds(m(o * OC, OC), OC)]

    AG_SEM = (0, 1, 2, 3, 4, 5, 6, 6, 7, 8, 7, 8, 9, 9)

    def ag_send(buf, k, slot, o, h, dev):
        view = part(buf, o, h)
        pltpu.make_async_remote_copy(
            src_ref=view, dst_ref=view, send_sem=agsend.at[k], recv_sem=agrecv.at[k, AG_SEM[slot]],
            device_id={"tp": dev}, device_id_type=MESH,
        ).start()

    def ag_start(buf, k):
        for slot, h, dev in ((0, 0, tr), (2, 1, tl), (1, 1, tr), (3, 0, tl), (6, 0, sib), (7, 1, sib)):
            ag_send(buf, k, slot, t, h, dev)

    SRC = {0: (tl, 0), 1: (tl, 1), 2: (tr, 1), 3: (tr, 0), 4: (2 * chip_2 + c, 0), 5: (2 * chip_2 + c, 1)}

    def ag_take(buf, k, slots):
        for slot in slots:
            o, h = SRC[slot]
            arrived(agrecv.at[k, AG_SEM[slot]], part(buf, o, h))
            if slot == 0:
                ag_send(buf, k, 4, o, h, tr)
            if slot == 2:
                ag_send(buf, k, 5, o, h, tl)
            ag_send(buf, k, slot + 8, o, h, sib)

    SIB_SRC = {6: (sib, 0), 7: (sib, 1)}
    SIB_SRC.update({slot + 8: (o + 1 - 2 * c, h) for slot, (o, h) in SRC.items()})

    def ag_end(buf, k, pairs=((6, 7), (8, 10), (9, 11), (12, 13)), then=lambda o, h: None):
        for pair in pairs:
            arrived(agrecv.at[k, AG_SEM[pair[0]]], buf.at[:, 0:OC])
            for slot in pair:
                then(*SIB_SRC[slot])

    ag_start(X, 0)
    loads[9].wait()
    x32 = xb[...].astype(F32)
    ss_store(0, [jnp.sum(x32 * x32, axis=1, keepdims=True)])
    for i in range(4, 9):
        loads[i].wait()
    NL = D // 128

    tick("A", 1)
    ss_start(0)
    own_sends("B")
    tick("A", 2)
    ag_take(X, 0, (0, 2))
    tick("A", 3)
    ag_take(X, 0, (1, 3))
    tick("B", 1, True)
    tick("A", 4)
    tick("B", 2, True)
    ag_take(X, 0, (4, 5))
    tick("A", 5)
    tick("B", 3, True)
    ag_end(X, 0)
    total0 = ss_total(0)
    r1, _ = columns(lax.rsqrt(total0[0:8] / D + EPS))
    tick("A", 6)
    scale_into(r1, g1_ref, 0, NL // 2)
    tick("B", 4, True)
    tick("A", 7)
    scale_into(r1, g1_ref, NL // 2, NL)
    tick("B", 5, True)
    tick("A", 8)
    y_flush()
    tick("B", 6)
    y_all("A")
    own_sends("P")

    qk = mm(XG[...], wqkv[:, 0 : 2 * KD])
    q = qk[:, 0:KD].astype(BF16).astype(F32) * KD ** (-0.5)
    k = qk[:, KD : 2 * KD].astype(BF16).astype(F32)
    v = mm(XG[...], wqkv[:, 2 * KD : 2 * KD + VD]).astype(BF16)
    tick("B", 7)
    own_sends("Q")
    low = mm_nt(XG[...], left_ref[...])
    low_hi, low_lo = split2(low)
    right_hi, right_lo = split2(right_ref[...])
    pre = mm(low_hi, right_hi) + (mm(low_lo, right_hi) + mm(low_hi, right_lo)) + const_ref[...]
    ld = (jnp.minimum(pre, 0.0) - jnp.log1p(jnp.exp(-jnp.abs(pre)))) / STEEPNESS + exc[...]

    ri = lax.broadcasted_iota(jnp.int32, (128, 128), 0)
    tri = jnp.where(ri >= lane_iota, 1.0, 0.0).astype(BF16)
    ld_hi, ld_lo = split2(ld)
    pieces, carry = [], jnp.zeros((1, KD), F32)
    for j in range(T // 128):
        rows = slice(j * 128, (j + 1) * 128)
        run = mm(tri, ld_hi[rows]) + mm(tri, ld_lo[rows]) + carry
        carry = run[127:128]
        pieces.append(run)
    b = jnp.concatenate(pieces, axis=0)
    tick("B", 8)
    tick("P", 1)
    own_sends("D")

    def offsets(span):
        b3 = b.reshape(T // span, span, KD)
        return (b3 - b3[:, span // 2 - 1 : span // 2, :]).reshape(T, KD)

    def level(span):
        d = offsets(span)
        second = lax.rem(row_iota, span) >= span // 2
        e = jnp.exp(jnp.where(second, d, -d))
        return jnp.where(second, q * e, 0.0).astype(BF16), jnp.where(second, 0.0, k * e).astype(BF16)

    dd = offsets(32)
    qd_hi, qd_lo = split2(q * jnp.exp(dd))
    kd_hi, kd_lo = split2(k * jnp.exp(-dd))
    qd = jnp.concatenate([qd_hi, qd_lo, qd_hi], axis=1)
    kd = jnp.concatenate([kd_hi, kd_hi, kd_lo], axis=1)
    q64, k64 = level(64)
    q128, k128 = level(128)
    q256, k256 = level(256)
    q512, k512 = level(512)
    tick("Q", 1)
    ci_ = lane_iota
    in32 = (ri // 32 == ci_ // 32) & (ri >= ci_)
    in64 = (ri // 64 == ci_ // 64) & (ri // 32 != ci_ // 32)
    diag = []
    for j in range(T // 128):
        rows = slice(j * 128, (j + 1) * 128)
        s = jnp.where(in32, mm_nt(qd[rows], kd[rows]), 0.0)
        s = s + jnp.where(in64, mm_nt(q64[rows], k64[rows]), 0.0)
        s = s + mm_nt(q128[rows], k128[rows])
        diag.append(s.astype(BF16))
    zero128 = jnp.zeros((128, 128), BF16)
    halves = []
    for j in range(2):
        lo = slice(j * 256, j * 256 + 128)
        hi = slice(j * 256 + 128, (j + 1) * 256)
        cross = mm_nt(q256[hi], k256[lo]).astype(BF16)
        top = mm(diag[2 * j], v[lo])
        bottom = mm(jnp.concatenate([cross, diag[2 * j + 1]], axis=1), v[j * 256 : (j + 1) * 256])
        halves.append(jnp.concatenate([top, bottom], axis=0))
    far = mm_nt(q512[256:512], k512[0:256]).astype(BF16)
    heads = jnp.concatenate([halves[0], halves[1] + mm(far, v[0:256])], axis=0)
    hs = lax.rsqrt(jnp.mean(heads * heads, axis=1, keepdims=True) + EPS)
    hout[...] = (heads * hs * egn_ref[...]).astype(BF16)
    tick("P", 2)
    y_all("B")

    def rs(k, lhs_ref, w, between):
        order = (chip_2, chip_r, chip_l, xi)

        def products(n):
            so[k, n] = mm(lhs_ref[...], w[2 * order[n] + 1 - c]).astype(BF16)
            acc[n] = mm(lhs_ref[...], w[2 * order[n] + c])
            pltpu.make_async_remote_copy(
                src_ref=so.at[k, n], dst_ref=si.at[k, n], send_sem=sibsend.at[k], recv_sem=sibrecv.at[k, n],
                device_id={"tp": sib}, device_id_type=MESH,
            ).start()

        def send(sem, src, dst, dev):
            pltpu.make_async_remote_copy(
                src_ref=src, dst_ref=dst, send_sem=rssend.at[k], recv_sem=rsrecv.at[k, sem],
                device_id={"tp": dev}, device_id_type=MESH,
            ).start()

        def with_sib(n, rows):
            return acc[n, rows, :] + si[k, n, rows, :].astype(F32)

        lo, hi = pl.ds(0, H), pl.ds(H, H)
        products(0)
        products(1)
        between(0)
        arrived(sibrecv.at[k, 0], si.at[k, 0])
        o2[k, lo, :] = with_sib(0, lo).astype(BF16)
        o2[k, hi, :] = with_sib(0, hi).astype(BF16)
        settle(o2[k, hi, :])
        send(0, o2.at[k, lo], ih.at[k, 0], tr)
        send(1, o2.at[k, hi], ih.at[k, 1], tl)
        between(1)
        products(2)
        arrived(sibrecv.at[k, 1], si.at[k, 1])
        orr[k, hi, :] = with_sib(1, hi).astype(BF16)
        between(2)
        products(3)
        send(2, orr.at[k, hi], ifl.at[k, 0, hi], tr)
        arrived(sibrecv.at[k, 2], si.at[k, 2])
        oll[k, lo, :] = with_sib(2, lo).astype(BF16)
        acc[1, lo, :] = with_sib(1, lo)
        acc[2, hi, :] = with_sib(2, hi)
        settle(oll[k, lo, :])
        send(2, oll.at[k, lo], ifl.at[k, 1, lo], tl)
        between(3)
        arrived(rsrecv.at[k, 0], ih.at[k, 0])
        orr[k, lo, :] = (acc[1, lo, :] + ih[k, 0].astype(F32)).astype(BF16)
        arrived(rsrecv.at[k, 1], ih.at[k, 1])
        oll[k, hi, :] = (acc[2, hi, :] + ih[k, 1].astype(F32)).astype(BF16)
        settle(orr[k, lo, :])
        send(3, orr.at[k, lo], ifl.at[k, 0, lo], tr)
        arrived(sibrecv.at[k, 3], si.at[k, 3])
        settle(oll[k, hi, :])
        send(3, oll.at[k, hi], ifl.at[k, 1, hi], tl)
        acc[3] = acc[3] + si[k, 3].astype(F32)
        between(4)
        arrived(rsrecv.at[k, 2], ifl.at[k, 0])
        between(5)
        arrived(rsrecv.at[k, 3], ifl.at[k, 0])
        return acc[3] + (ifl[k, 0].astype(F32) + ifl[k, 1].astype(F32))

    WORK = (("Q2",), ("D1",), ("P3",), ("Q3", "P4"), ("D2", "Q4"), ("P5", "D3"))

    def ticks(*names):
        for name in names:
            tick(name[0], int(name[1]))

    def between0(i):
        ticks(*WORK[i])

    mixed = rs(0, hout, wc, between0)
    mg = mixed * gain_row(gaf_ref)
    F[:, pl.ds(m(t * OC, OC), OC)] = mg.astype(BF16)
    x32 = xb[...].astype(F32)
    ss_store(1, [jnp.sum(a, axis=1, keepdims=True) for a in (mixed * mixed, x32 * mg, mg * mg)])
    ss_start(1)
    settle(F[H:T, pl.ds(m(t * OC, OC), OC)])
    ag_start(F, 1)
    acc[3] = mg
    ticks("Q5", "P6", "D4")
    ag_take(F, 1, (0, 2))
    ticks("Q6")
    total1 = ss_total(1)
    ra_rows = lax.rsqrt(total1[0:NB] / D + EPS)
    squares = total0[0:NB] + 2.0 * ra_rows * total1[NB : 2 * NB] + ra_rows * ra_rows * total1[2 * NB : 3 * NB]
    ra, r2 = columns(jnp.concatenate([ra_rows, lax.rsqrt(squares / D + EPS)], axis=0))
    firstb[...] = (x32 + acc[3] * ra).astype(BF16)

    def join(o, h):
        rows, cols = pl.ds(h * H, H), pl.ds(m(o * OC, OC), OC)
        gain = jnp.concatenate([gdi_ref[pl.ds(o * (OC // 128) + i, 1), :] for i in range(OC // 128)], axis=1)
        whole = X[rows, cols].astype(F32) + F[rows, cols].astype(F32) * ra[h * H : (h + 1) * H]
        XG[rows, cols] = (whole * gain).astype(BF16)

    join(t, 0)
    join(t, 1)
    join(*SRC[0])
    join(*SRC[2])
    ag_end(F, 1, ((6, 7),), join)
    ticks("P7", "D5")
    ag_take(F, 1, (1, 3))
    ticks("Q7")
    join(*SRC[1])
    join(*SRC[3])
    ag_end(F, 1, ((8, 10),), join)
    ticks("P8", "D6")
    ag_take(F, 1, (4, 5))
    ticks("Q8")
    join(*SRC[4])
    join(*SRC[5])
    ag_end(F, 1, ((9, 11),), join)
    ag_end(F, 1, ((12, 13),), join)
    ticks("D7")
    y_all("P")

    PAD = 8
    G[0:PAD, :] = jnp.zeros((PAD, 2 * FU), F32)
    for n in range(2 * FU // 256):
        cols = slice(n * 256, (n + 1) * 256)
        G[PAD : PAD + T, cols] = mm(XG[...], wgu[:, cols]) * r2
        if n == 1:
            tick("D", 8)

    def taps(ref, base):
        w = ref[:, base % FU : base % FU + 128].astype(F32)
        n = w.shape[0]
        total = None
        for j in range(n):
            term = w[j : j + 1] * G[PAD - (n - 1) + j : PAD - (n - 1) + j + T, base : base + 128]
            total = term if total is None else total + term
        return total

    for n in range(FU // 128):
        gc, uc = taps(tapg_ref, n * 128), taps(tapu_ref, FU + n * 128)
        hidden[:, n * 128 : (n + 1) * 128] = (gc / (1.0 + jnp.exp(-gc)) * uc).astype(BF16)
    y_all("D")
    channel = rs(1, hidden, wd, lambda i: None)
    ss_store(2, [jnp.sum(channel * channel, axis=1, keepdims=True)])
    acc[3] = channel
    ss_start(2)
    for i, name in enumerate(NAMES):
        for d in (0, 1):
            left(zsend.at[d, i], block(sent_z[d, name]))
        if sent_y[name]:
            left(ysend.at[i], block(sent_y[name]))
    for k in (0, 1):
        left(agsend.at[k], X.at[0 : 14 * H * OC // D, :])
        left(sibsend.at[k], so.at[k])
        left(rssend.at[k], X.at[0 : 6 * H * OC // D, :])
        left(sssend.at[k], ss.at[k, 0 : NTP - 1])
    rc, _ = columns(lax.rsqrt(ss_total(2)[0:8] / D + EPS))
    out_ref[...] = (firstb[...].astype(F32) + acc[3] * rc * gain_row(gdf_ref)).astype(BF16)
    left(sssend.at[2], ss.at[2, 0 : NTP - 1])


def on_device(
    dims, x, g1, egn, gaf, gdi, gdf, wq, wk, wv, left, right, const, excess, comb, gate, up, tapg, tapu, down
):
    NG, NZ, NTP = dims
    T, OC = x.shape
    D = OC * NTP
    KD, VD, FU = wq.shape[1], wv.shape[1], gate.shape[1]
    any_ = pl.BlockSpec(memory_space=pl.ANY)
    vm = pl.BlockSpec(memory_space=pltpu.VMEM)
    DMA = pltpu.SemaphoreType.DMA
    NX = NTP // 2
    VM = pltpu.VMEM
    scratch = [
        VM((8, 128), F32), VM((T, OC), BF16), VM((T, D), BF16), VM((T, D), BF16), VM((T, D), BF16),
        VM((D, 2 * KD + VD), BF16), VM((NTP, comb.shape[0], OC), BF16), VM((D, 2 * FU), BF16), VM((NTP, FU, OC), BF16),
        VM((T, KD), F32), VM((3, NTP, 16, 128), F32),
        VM((T, VD), BF16), VM((T, FU), BF16), VM((T + 8, 2 * FU), F32), VM((T, OC), BF16),
        VM((NX, T, OC), F32), VM((2, NX, T, OC), BF16), VM((2, NX, T, OC), BF16),
        VM((2, T, OC), BF16), VM((2, T, OC), BF16), VM((2, T, OC), BF16),
        VM((2, 2, T // 2, OC), BF16), VM((2, 2, T, OC), BF16),
        DMA((10,)), DMA((14, NZ // 2)), DMA((2, 5)), DMA((5,)), DMA((5,)),
        DMA((2, 10)), DMA((2,)), DMA((3,)), DMA((3,)), DMA((2, NX)), DMA((2,)), DMA((2, 4)), DMA((2,)),
    ]
    return pl.pallas_call(
        functools.partial(layer_kernel, dims),
        out_shape=jax.ShapeDtypeStruct((T, OC), BF16),
        in_specs=[any_] * 9 + [vm] * 10,
        out_specs=vm,
        scratch_shapes=scratch,
        compiler_params=pltpu.CompilerParams(
            collective_id=0, has_side_effects=True, vmem_limit_bytes=60 * 1024 * 1024
        ),
        name="layer",
    )(
        x, wq, wk, wv, comb, gate, up, down, excess,
        g1.reshape(-1, 128), gaf.reshape(-1, 128), gdi.reshape(-1, 128), gdf.reshape(-1, 128),
        egn, left.T, right, const.reshape(1, -1), tapg, tapu,
    )


def solution(mesh):
    dims = (mesh.shape["grp"], mesh.shape["fs"], mesh.shape["tp"])
    placed = (
        P(("grp", "fs"), "tp"), P(), P("tp", None), P(), P(), P(), P("fs", "tp"), P("fs", "tp"), P("fs", "tp"), P(),
        P(None, "tp"), P("tp"), P(("grp", "fs"), "tp"), P("tp", "fs"), P("fs", "tp"), P("fs", "tp"), P(None, "tp"),
        P(None, "tp"), P("tp", "fs"),
    )
    return jax.shard_map(
        functools.partial(on_device, dims), mesh=mesh, in_specs=placed, out_specs=P(("grp", "fs"), "tp"),
        check_vma=False,
    )
```

```python
import functools

import jax
import jax.numpy as jnp
from jax import lax
from jax.experimental import pallas as pl
from jax.experimental.pallas import tpu as pltpu
from jax.sharding import PartitionSpec as P

EPS = 1e-06
STEEPNESS = 16.0
MESH = pl.DeviceIdType.MESH
F32 = jnp.float32
BF16 = jnp.bfloat16
NEG = -1e30


def mm(a, b):
    return jnp.dot(a, b, preferred_element_type=F32)


def mm_nt(a, b):
    return lax.dot_general(a, b, (((1,), (1,)), ((), ())), preferred_element_type=F32)


def split2(v):
    hi = v.astype(BF16)
    return hi, (v - hi.astype(F32)).astype(BF16)


def layer_kernel(
    dims,
    x_hbm, q_hbm, k_hbm, v_hbm, comb_hbm, gate_hbm, up_hbm, down_hbm, exc_hbm,
    g1_ref, gaf_ref, gdi_ref, gdf_ref, egn_ref, left_ref, right_ref, const_ref, tapg_ref, tapu_ref,
    out_ref,
    back, xb, X, XG, F, wqkv, wc, wgu, wd, exc, ss, hout, hidden, G, firstb, acc, so, si, o2, orr, oll, ih, ifl,
    local_sem, zrecv, zsend, yrecv, ysend, agrecv, agsend, ssrecv, sssend, sibrecv, sibsend, rsrecv, rssend,
):
    NG, NZ, NTP = dims
    T, OC = xb.shape
    D = X.shape[1]
    NX = NTP // 2
    KD = q_hbm.shape[1]
    VD = v_hbm.shape[1]
    FU = gate_hbm.shape[1]
    RZ = q_hbm.shape[0]
    CZ = comb_hbm.shape[1]
    PER = OC // CZ
    H = T // 2
    HALF = NZ // 2

    g, z, t = lax.axis_index("grp"), lax.axis_index("fs"), lax.axis_index("tp")
    par = lax.rem(g, 2)
    pg = g + 1 - 2 * par
    xi, c = t // 2, lax.rem(t, 2)
    chip_r, chip_l, chip_2 = lax.rem(xi + 1, NX), lax.rem(xi + NX - 1, NX), lax.rem(xi + 2, NX)
    sib = 2 * xi + 1 - c
    tr, tl = 2 * chip_r + c, 2 * chip_l + c
    zr, zl = lax.rem(z + 1, NZ), lax.rem(z + NZ - 1, NZ)

    def m(v, n):
        return pl.multiple_of(v, n)

    def wview(ref, o, r0, rows):
        return ref.at[pl.ds(m(o * RZ + r0, 16), rows), :]

    def cview(ref, o, r0, rows):
        return ref.at[o // PER, pl.ds(m(r0, 16), rows), pl.ds(m(lax.rem(o, PER) * CZ, CZ), CZ)]

    VR = comb_hbm.shape[0]
    b_m, b_c = 96, VR - 192
    d_m, d_c = 144, FU - 288
    W = 2 * KD + VD
    PHASES = {
        "A": [(lambda o, p, i=i: wview(wqkv, o, p * 48 + 16 * i, 16), True, 16 * W) for i in range(3)]
        + [(lambda o, p, i=i: wview(wqkv, o, 96 + 16 * i, 16), False, 16 * W) for i in range((RZ - 96) // 16)],
        "B": [
            (lambda o, p: cview(wc, o, p * b_m, b_m), True, b_m * CZ),
            (lambda o, p: cview(wc, o, 2 * b_m, b_c), False, b_c * CZ),
        ],
        "P": [(lambda o, p, i=i: wview(wgu, o, p * 48 + 16 * i, 16), True, 16 * 2 * FU) for i in range(3)],
        "Q": [(lambda o, p, i=i: wview(wgu, o, 96 + 16 * i, 16), False, 16 * 2 * FU) for i in range((RZ - 96) // 16)],
        "D": [
            (lambda o, p: cview(wd, o, p * d_m, d_m), True, d_m * CZ),
            (lambda o, p: cview(wd, o, 2 * d_m, d_c), False, d_c * CZ),
        ],
    }
    ANTIPODE = {"A": ((0, 2, 4), (1, 3)), "B": ((0,), (1,)), "P": ((0,), (1, 2)), "Q": ((0,), (1,)), "D": ((0,), (1,))}
    NAMES = list(PHASES)
    ZBASE, zn = {}, 0
    for name, chunks in PHASES.items():
        ZBASE[name] = zn
        zn += len(chunks)

    def block(elements):
        for ref, wide in ((wgu, 2 * FU), (wqkv, W), (wgu, FU), (wqkv, 128)):
            rows = elements // wide
            if elements % (16 * wide) == 0 and rows <= D:
                return ref.at[0:rows, 0:wide]
        raise ValueError(elements)

    def arrived(sem, view):
        pltpu.make_async_remote_copy(
            src_ref=view, dst_ref=view, send_sem=sem, recv_sem=sem, device_id={"tp": sib}, device_id_type=MESH
        ).wait_recv()

    def left(sem, view):
        pltpu.make_async_remote_copy(
            src_ref=view, dst_ref=view, send_sem=sem, recv_sem=sem, device_id={"tp": sib}, device_id_type=MESH
        ).wait_send()

    sent_z = {(d, n): 0 for d in (0, 1) for n in NAMES}
    sent_y = {n: 0 for n in NAMES}

    def steps_from(d, s):
        return lax.rem(z + NZ - s, NZ) if d == 0 else lax.rem(z + s, NZ)

    def zstart(phase, ci, d, hop):
        view = PHASES[phase][ci][0](steps_from(d, hop), par)
        pltpu.make_async_remote_copy(
            src_ref=view, dst_ref=view,
            send_sem=zsend.at[d, NAMES.index(phase)], recv_sem=zrecv.at[ZBASE[phase] + ci, hop],
            device_id={"fs": zr if d == 0 else zl}, device_id_type=MESH,
        ).start()
        sent_z[d, phase] += PHASES[phase][ci][2]

    def ystart(phase, ci, d, s):
        view = PHASES[phase][ci][0](steps_from(d, s), par)
        i = NAMES.index(phase)
        pltpu.make_async_remote_copy(
            src_ref=view, dst_ref=view, send_sem=ysend.at[i], recv_sem=yrecv.at[i],
            device_id={"grp": pg}, device_id_type=MESH,
        ).start()
        sent_y[phase] += PHASES[phase][ci][2]

    def own_sends(phase):
        for ci in range(len(PHASES[phase])):
            for d in (0, 1):
                zstart(phase, ci, d, 0)

    deferred = []

    def y_flush():
        for args in deferred:
            ystart(*args)
        deferred.clear()

    def tick(phase, s, hold=False):
        for ci, (_, exchanged, elements) in enumerate(PHASES[phase]):
            dirs = [d for d in (0, 1) if s < HALF or ci in ANTIPODE[phase][d]]
            arrived(zrecv.at[ZBASE[phase] + ci, s - 1], block(elements * len(dirs)))
            for d in dirs:
                if s < HALF - 1 or (s == HALF - 1 and ci in ANTIPODE[phase][d]):
                    zstart(phase, ci, d, s)
            for d in dirs:
                if exchanged and hold:
                    deferred.append((phase, ci, d, s))
                elif exchanged:
                    ystart(phase, ci, d, s)

    def y_all(phase):
        arrived(yrecv.at[NAMES.index(phase)], block(sum(n for _, e, n in PHASES[phase] if e) * (NZ - 1)))

    zo = z
    locals_ = [
        (x_hbm, X.at[:, pl.ds(m(t * OC, OC), OC)]),
        (q_hbm, wqkv.at[pl.ds(m(zo * RZ, 16), RZ), 0:KD]),
        (k_hbm, wqkv.at[pl.ds(m(zo * RZ, 16), RZ), KD : 2 * KD]),
        (v_hbm, wqkv.at[pl.ds(m(zo * RZ, 16), RZ), 2 * KD : 2 * KD + VD]),
        (comb_hbm, cview(wc, zo, 0, VR)),
        (gate_hbm, wgu.at[pl.ds(m(zo * RZ, 16), RZ), 0:FU]),
        (up_hbm, wgu.at[pl.ds(m(zo * RZ, 16), RZ), FU : 2 * FU]),
        (down_hbm, cview(wd, zo, 0, FU)),
        (exc_hbm, exc),
        (x_hbm, xb),
    ]
    loads = [pltpu.make_async_copy(a, b, local_sem.at[i]) for i, (a, b) in enumerate(locals_)]
    for copy in loads:
        copy.start()

    back[...] = jnp.zeros_like(back)

    barrier = pltpu.get_barrier_semaphore()
    for d in range(1, NTP):
        pl.semaphore_signal(barrier, inc=1, device_id={"tp": lax.rem(t + d, NTP)}, device_id_type=MESH)
    for other in (zr, zl):
        pl.semaphore_signal(barrier, inc=1, device_id={"fs": other}, device_id_type=MESH)
    pl.semaphore_signal(barrier, inc=1, device_id={"grp": pg}, device_id_type=MESH)
    for i in range(0, 4):
        loads[i].wait()
    pl.semaphore_wait(barrier, NTP + 2)
    own_sends("A")

    row_iota = lax.broadcasted_iota(jnp.int32, (T, 1), 0)
    lane_iota = lax.broadcasted_iota(jnp.int32, (128, 128), 1)

    def gain_row(ref):
        per = OC // 128
        rows = [ref[pl.ds(t * per + i, 1), :] for i in range(per)]
        return jnp.concatenate(rows, axis=1)

    NB = T // 128

    def ss_store(k, cols):
        mat = jnp.zeros((128, 128), F32)
        for i, col in enumerate(cols):
            for j in range(NB):
                mat = jnp.where(lane_iota == i * NB + j, col[j * 128 : (j + 1) * 128], mat)
        ss[k, t] = mat.T[0:16, :]

    def settle(block_):
        rows = 16 if block_.dtype == BF16 else 8
        got = block_.reshape(-1, rows, block_.shape[-1])
        back[...] = back[...] + jnp.max(got, axis=0)[0:8, 0:128].astype(F32)

    def ss_start(k):
        settle(ss[k, t])
        for d in range(1, NTP):
            pltpu.make_async_remote_copy(
                src_ref=ss.at[k, t], dst_ref=ss.at[k, t], send_sem=sssend.at[k], recv_sem=ssrecv.at[k],
                device_id={"tp": lax.rem(t + d, NTP)}, device_id_type=MESH,
            ).start()

    def ss_total(k):
        arrived(ssrecv.at[k], ss.at[k, 0 : NTP - 1])
        total = ss[k, 0]
        for i in range(1, NTP):
            total = total + ss[k, i]
        return total

    def columns(rows):
        cols = jnp.concatenate([rows, jnp.zeros((120, 128), F32)], axis=0).T
        pick = lambda a: jnp.concatenate([cols[:, a + j : a + j + 1] for j in range(NB)], axis=0)
        return pick(0), pick(NB)

    def scale_into(scale, ref, lo, hi):
        for l in range(lo, hi):
            cols = slice(l * 128, (l + 1) * 128)
            XG[:, cols] = (X[:, cols].astype(F32) * scale * ref[l : l + 1, :]).astype(BF16)

    def part(buf, o, h):
        return buf.at[pl.ds(h * H, H), pl.ds(m(o * OC, OC), OC)]

    AG_SEM = (0, 1, 2, 3, 4, 5, 6, 6, 7, 8, 7, 8, 9, 9)

    def ag_send(buf, k, slot, o, h, dev):
        view = part(buf, o, h)
        pltpu.make_async_remote_copy(
            src_ref=view, dst_ref=view, send_sem=agsend.at[k], recv_sem=agrecv.at[k, AG_SEM[slot]],
            device_id={"tp": dev}, device_id_type=MESH,
        ).start()

    def ag_start(buf, k):
        for slot, h, dev in ((0, 0, tr), (2, 1, tl), (1, 1, tr), (3, 0, tl), (6, 0, sib), (7, 1, sib)):
            ag_send(buf, k, slot, t, h, dev)

    SRC = {0: (tl, 0), 1: (tl, 1), 2: (tr, 1), 3: (tr, 0), 4: (2 * chip_2 + c, 0), 5: (2 * chip_2 + c, 1)}

    def ag_take(buf, k, slots):
        for slot in slots:
            o, h = SRC[slot]
            arrived(agrecv.at[k, AG_SEM[slot]], part(buf, o, h))
            if slot == 0:
                ag_send(buf, k, 4, o, h, tr)
            if slot == 2:
                ag_send(buf, k, 5, o, h, tl)
            ag_send(buf, k, slot + 8, o, h, sib)

    SIB_SRC = {6: (sib, 0), 7: (sib, 1)}
    SIB_SRC.update({slot + 8: (o + 1 - 2 * c, h) for slot, (o, h) in SRC.items()})

    def ag_end(buf, k, pairs=((6, 7), (8, 10), (9, 11), (12, 13)), then=lambda o, h: None):
        for pair in pairs:
            arrived(agrecv.at[k, AG_SEM[pair[0]]], buf.at[:, 0:OC])
            for slot in pair:
                then(*SIB_SRC[slot])

    ag_start(X, 0)
    loads[9].wait()
    x32 = xb[...].astype(F32)
    ss_store(0, [jnp.sum(x32 * x32, axis=1, keepdims=True)])
    for i in range(4, 9):
        loads[i].wait()
    NL = D // 128

    tick("A", 1)
    ss_start(0)
    own_sends("B")
    tick("A", 2)
    tick("B", 1, True)
    ag_take(X, 0, (0, 2))
    tick("A", 3)
    tick("B", 2, True)
    ag_take(X, 0, (1, 3))
    tick("A", 4)
    tick("B", 3, True)
    ag_take(X, 0, (4, 5))
    tick("A", 5)
    tick("B", 4, True)
    ag_end(X, 0)
    total0 = ss_total(0)
    r1, _ = columns(lax.rsqrt(total0[0:8] / D + EPS))
    tick("A", 6)
    scale_into(r1, g1_ref, 0, NL // 2)
    tick("B", 5, True)
    tick("A", 7)
    scale_into(r1, g1_ref, NL // 2, NL)
    tick("B", 6, True)
    tick("A", 8)
    y_flush()
    tick("B", 7)
    y_all("A")
    own_sends("P")

    qk = mm(XG[...], wqkv[:, 0 : 2 * KD])
    q = qk[:, 0:KD].astype(BF16).astype(F32) * KD ** (-0.5)
    k = qk[:, KD : 2 * KD].astype(BF16).astype(F32)
    v = mm(XG[...], wqkv[:, 2 * KD : 2 * KD + VD]).astype(BF16)
    tick("B", 8)
    own_sends("Q")
    low = mm_nt(XG[...], left_ref[...])
    low_hi, low_lo = split2(low)
    right_hi, right_lo = split2(right_ref[...])
    pre = mm(low_hi, right_hi) + (mm(low_lo, right_hi) + mm(low_hi, right_lo)) + const_ref[...]
    ld = (jnp.minimum(pre, 0.0) - jnp.log1p(jnp.exp(-jnp.abs(pre)))) / STEEPNESS + exc[...]

    ri = lax.broadcasted_iota(jnp.int32, (128, 128), 0)
    tri = jnp.where(ri >= lane_iota, 1.0, 0.0).astype(BF16)
    ld_hi, ld_lo = split2(ld)
    pieces, carry = [], jnp.zeros((1, KD), F32)
    for j in range(T // 128):
        rows = slice(j * 128, (j + 1) * 128)
        run = mm(tri, ld_hi[rows]) + mm(tri, ld_lo[rows]) + carry
        carry = run[127:128]
        pieces.append(run)
    b = jnp.concatenate(pieces, axis=0)
    tick("P", 1)
    own_sends("D")

    def offsets(span):
        b3 = b.reshape(T // span, span, KD)
        return (b3 - b3[:, span // 2 - 1 : span // 2, :]).reshape(T, KD)

    def level(span):
        d = offsets(span)
        second = lax.rem(row_iota, span) >= span // 2
        e = jnp.exp(jnp.where(second, d, -d))
        return jnp.where(second, q * e, 0.0).astype(BF16), jnp.where(second, 0.0, k * e).astype(BF16)

    dd = offsets(32)
    qd_hi, qd_lo = split2(q * jnp.exp(dd))
    kd_hi, kd_lo = split2(k * jnp.exp(-dd))
    qd = jnp.concatenate([qd_hi, qd_lo, qd_hi], axis=1)
    kd = jnp.concatenate([kd_hi, kd_hi, kd_lo], axis=1)
    q64, k64 = level(64)
    q128, k128 = level(128)
    q256, k256 = level(256)
    q512, k512 = level(512)
    tick("Q", 1)
    ci_ = lane_iota
    in32 = (ri // 32 == ci_ // 32) & (ri >= ci_)
    in64 = (ri // 64 == ci_ // 64) & (ri // 32 != ci_ // 32)
    diag = []
    for j in range(T // 128):
        rows = slice(j * 128, (j + 1) * 128)
        s = jnp.where(in32, mm_nt(qd[rows], kd[rows]), 0.0)
        s = s + jnp.where(in64, mm_nt(q64[rows], k64[rows]), 0.0)
        s = s + mm_nt(q128[rows], k128[rows])
        diag.append(s.astype(BF16))
    zero128 = jnp.zeros((128, 128), BF16)
    halves = []
    for j in range(2):
        lo = slice(j * 256, j * 256 + 128)
        hi = slice(j * 256 + 128, (j + 1) * 256)
        cross = mm_nt(q256[hi], k256[lo]).astype(BF16)
        top = mm(diag[2 * j], v[lo])
        bottom = mm(jnp.concatenate([cross, diag[2 * j + 1]], axis=1), v[j * 256 : (j + 1) * 256])
        halves.append(jnp.concatenate([top, bottom], axis=0))
    far = mm_nt(q512[256:512], k512[0:256]).astype(BF16)
    heads = jnp.concatenate([halves[0], halves[1] + mm(far, v[0:256])], axis=0)
    hs = lax.rsqrt(jnp.mean(heads * heads, axis=1, keepdims=True) + EPS)
    hout[...] = (heads * hs * egn_ref[...]).astype(BF16)
    tick("P", 2)
    y_all("B")

    def rs(k, lhs_ref, w, between):
        order = (chip_2, chip_r, chip_l, xi)

        def products(n):
            so[k, n] = mm(lhs_ref[...], w[2 * order[n] + 1 - c]).astype(BF16)
            acc[n] = mm(lhs_ref[...], w[2 * order[n] + c])
            pltpu.make_async_remote_copy(
                src_ref=so.at[k, n], dst_ref=si.at[k, n], send_sem=sibsend.at[k], recv_sem=sibrecv.at[k, n],
                device_id={"tp": sib}, device_id_type=MESH,
            ).start()

        def send(sem, src, dst, dev):
            pltpu.make_async_remote_copy(
                src_ref=src, dst_ref=dst, send_sem=rssend.at[k], recv_sem=rsrecv.at[k, sem],
                device_id={"tp": dev}, device_id_type=MESH,
            ).start()

        def with_sib(n, rows):
            return acc[n, rows, :] + si[k, n, rows, :].astype(F32)

        lo, hi = pl.ds(0, H), pl.ds(H, H)
        products(0)
        products(1)
        between(0)
        arrived(sibrecv.at[k, 0], si.at[k, 0])
        o2[k, lo, :] = with_sib(0, lo).astype(BF16)
        o2[k, hi, :] = with_sib(0, hi).astype(BF16)
        settle(o2[k, hi, :])
        send(0, o2.at[k, lo], ih.at[k, 0], tr)
        send(1, o2.at[k, hi], ih.at[k, 1], tl)
        between(1)
        products(2)
        arrived(sibrecv.at[k, 1], si.at[k, 1])
        orr[k, hi, :] = with_sib(1, hi).astype(BF16)
        between(2)
        products(3)
        send(2, orr.at[k, hi], ifl.at[k, 0, hi], tr)
        arrived(sibrecv.at[k, 2], si.at[k, 2])
        oll[k, lo, :] = with_sib(2, lo).astype(BF16)
        acc[1, lo, :] = with_sib(1, lo)
        acc[2, hi, :] = with_sib(2, hi)
        settle(oll[k, lo, :])
        send(2, oll.at[k, lo], ifl.at[k, 1, lo], tl)
        between(3)
        arrived(rsrecv.at[k, 0], ih.at[k, 0])
        orr[k, lo, :] = (acc[1, lo, :] + ih[k, 0].astype(F32)).astype(BF16)
        arrived(rsrecv.at[k, 1], ih.at[k, 1])
        oll[k, hi, :] = (acc[2, hi, :] + ih[k, 1].astype(F32)).astype(BF16)
        settle(orr[k, lo, :])
        send(3, orr.at[k, lo], ifl.at[k, 0, lo], tr)
        arrived(sibrecv.at[k, 3], si.at[k, 3])
        settle(oll[k, hi, :])
        send(3, oll.at[k, hi], ifl.at[k, 1, hi], tl)
        acc[3] = acc[3] + si[k, 3].astype(F32)
        between(4)
        arrived(rsrecv.at[k, 2], ifl.at[k, 0])
        between(5)
        arrived(rsrecv.at[k, 3], ifl.at[k, 0])
        return acc[3] + (ifl[k, 0].astype(F32) + ifl[k, 1].astype(F32))

    WORK = (("Q2",), ("D1",), ("P3",), ("Q3", "P4"), ("D2", "Q4"), ("P5", "D3"))

    def ticks(*names):
        for name in names:
            tick(name[0], int(name[1]))

    def between0(i):
        ticks(*WORK[i])

    mixed = rs(0, hout, wc, between0)
    mg = mixed * gain_row(gaf_ref)
    F[:, pl.ds(m(t * OC, OC), OC)] = mg.astype(BF16)
    x32 = xb[...].astype(F32)
    ss_store(1, [jnp.sum(a, axis=1, keepdims=True) for a in (mixed * mixed, x32 * mg, mg * mg)])
    ss_start(1)
    settle(F[H:T, pl.ds(m(t * OC, OC), OC)])
    ag_start(F, 1)
    acc[3] = mg
    ticks("Q5", "P6", "D4")
    ag_take(F, 1, (0, 2))
    ticks("Q6")
    total1 = ss_total(1)
    ra_rows = lax.rsqrt(total1[0:NB] / D + EPS)
    squares = total0[0:NB] + 2.0 * ra_rows * total1[NB : 2 * NB] + ra_rows * ra_rows * total1[2 * NB : 3 * NB]
    ra, r2 = columns(jnp.concatenate([ra_rows, lax.rsqrt(squares / D + EPS)], axis=0))
    firstb[...] = (x32 + acc[3] * ra).astype(BF16)

    def join(o, h):
        rows, cols = pl.ds(h * H, H), pl.ds(m(o * OC, OC), OC)
        gain = jnp.concatenate([gdi_ref[pl.ds(o * (OC // 128) + i, 1), :] for i in range(OC // 128)], axis=1)
        whole = X[rows, cols].astype(F32) + F[rows, cols].astype(F32) * ra[h * H : (h + 1) * H]
        XG[rows, cols] = (whole * gain).astype(BF16)

    join(t, 0)
    join(t, 1)
    join(*SRC[0])
    join(*SRC[2])
    ag_end(F, 1, ((6, 7),), join)
    ticks("P7", "D5")
    ag_take(F, 1, (1, 3))
    ticks("Q7")
    join(*SRC[1])
    join(*SRC[3])
    ag_end(F, 1, ((8, 10),), join)
    ticks("P8", "D6")
    ag_take(F, 1, (4, 5))
    ticks("Q8")
    join(*SRC[4])
    join(*SRC[5])
    ag_end(F, 1, ((9, 11),), join)
    ag_end(F, 1, ((12, 13),), join)
    ticks("D7")
    y_all("P")

    PAD = 8
    G[0:PAD, :] = jnp.zeros((PAD, 2 * FU), F32)
    for n in range(2 * FU // 256):
        cols = slice(n * 256, (n + 1) * 256)
        G[PAD : PAD + T, cols] = mm(XG[...], wgu[:, cols]) * r2
        if n == 1:
            tick("D", 8)

    def taps(ref, base):
        w = ref[:, base % FU : base % FU + 128].astype(F32)
        n = w.shape[0]
        total = None
        for j in range(n):
            term = w[j : j + 1] * G[PAD - (n - 1) + j : PAD - (n - 1) + j + T, base : base + 128]
            total = term if total is None else total + term
        return total

    for n in range(FU // 128):
        gc, uc = taps(tapg_ref, n * 128), taps(tapu_ref, FU + n * 128)
        hidden[:, n * 128 : (n + 1) * 128] = (gc / (1.0 + jnp.exp(-gc)) * uc).astype(BF16)
    y_all("D")
    channel = rs(1, hidden, wd, lambda i: None)
    ss_store(2, [jnp.sum(channel * channel, axis=1, keepdims=True)])
    acc[3] = channel
    ss_start(2)
    for i, name in enumerate(NAMES):
        for d in (0, 1):
            left(zsend.at[d, i], block(sent_z[d, name]))
        if sent_y[name]:
            left(ysend.at[i], block(sent_y[name]))
    for k in (0, 1):
        left(agsend.at[k], X.at[0 : 14 * H * OC // D, :])
        left(sibsend.at[k], so.at[k])
        left(rssend.at[k], X.at[0 : 6 * H * OC // D, :])
        left(sssend.at[k], ss.at[k, 0 : NTP - 1])
    rc, _ = columns(lax.rsqrt(ss_total(2)[0:8] / D + EPS))
    out_ref[...] = (firstb[...].astype(F32) + acc[3] * rc * gain_row(gdf_ref)).astype(BF16)
    left(sssend.at[2], ss.at[2, 0 : NTP - 1])


def on_device(
    dims, x, g1, egn, gaf, gdi, gdf, wq, wk, wv, left, right, const, excess, comb, gate, up, tapg, tapu, down
):
    NG, NZ, NTP = dims
    T, OC = x.shape
    D = OC * NTP
    KD, VD, FU = wq.shape[1], wv.shape[1], gate.shape[1]
    any_ = pl.BlockSpec(memory_space=pl.ANY)
    vm = pl.BlockSpec(memory_space=pltpu.VMEM)
    DMA = pltpu.SemaphoreType.DMA
    NX = NTP // 2
    VM = pltpu.VMEM
    scratch = [
        VM((8, 128), F32), VM((T, OC), BF16), VM((T, D), BF16), VM((T, D), BF16), VM((T, D), BF16),
        VM((D, 2 * KD + VD), BF16), VM((NTP, comb.shape[0], OC), BF16), VM((D, 2 * FU), BF16), VM((NTP, FU, OC), BF16),
        VM((T, KD), F32), VM((3, NTP, 16, 128), F32),
        VM((T, VD), BF16), VM((T, FU), BF16), VM((T + 8, 2 * FU), F32), VM((T, OC), BF16),
        VM((NX, T, OC), F32), VM((2, NX, T, OC), BF16), VM((2, NX, T, OC), BF16),
        VM((2, T, OC), BF16), VM((2, T, OC), BF16), VM((2, T, OC), BF16),
        VM((2, 2, T // 2, OC), BF16), VM((2, 2, T, OC), BF16),
        DMA((10,)), DMA((14, NZ // 2)), DMA((2, 5)), DMA((5,)), DMA((5,)),
        DMA((2, 10)), DMA((2,)), DMA((3,)), DMA((3,)), DMA((2, NX)), DMA((2,)), DMA((2, 4)), DMA((2,)),
    ]
    return pl.pallas_call(
        functools.partial(layer_kernel, dims),
        out_shape=jax.ShapeDtypeStruct((T, OC), BF16),
        in_specs=[any_] * 9 + [vm] * 10,
        out_specs=vm,
        scratch_shapes=scratch,
        compiler_params=pltpu.CompilerParams(
            collective_id=0, has_side_effects=True, vmem_limit_bytes=60 * 1024 * 1024
        ),
        name="layer",
    )(
        x, wq, wk, wv, comb, gate, up, down, excess,
        g1.reshape(-1, 128), gaf.reshape(-1, 128), gdi.reshape(-1, 128), gdf.reshape(-1, 128),
        egn, left.T, right, const.reshape(1, -1), tapg, tapu,
    )


def solution(mesh):
    dims = (mesh.shape["grp"], mesh.shape["fs"], mesh.shape["tp"])
    placed = (
        P(("grp", "fs"), "tp"), P(), P("tp", None), P(), P(), P(), P("fs", "tp"), P("fs", "tp"), P("fs", "tp"), P(),
        P(None, "tp"), P("tp"), P(("grp", "fs"), "tp"), P("tp", "fs"), P("fs", "tp"), P("fs", "tp"), P(None, "tp"),
        P(None, "tp"), P("tp", "fs"),
    )
    return jax.shard_map(
        functools.partial(on_device, dims), mesh=mesh, in_specs=placed, out_specs=P(("grp", "fs"), "tp"),
        check_vma=False,
    )
```
